256 devices in a mesh: sp: 32 (over z, x), tp: 8 (over y, core).
Axes of the slice: x: 4, y: 4, z: 8, core: 2. Of those that a mesh axis runs over, the one named last changes fastest.
Arguments:
- residual: bfloat16 [24576, 2048], P('sp'), may hold values from -6 to 6
- queries: bfloat16 [24576, 1024], P('sp', 'tp'), may hold values from -12 to 12
- keys: bfloat16 [24576, 512], P('sp', 'tp'), may hold values from -6 to 6
- values: bfloat16 [24576, 512], P('sp', 'tp'), may hold values from -36 to 36
- segments: int32 [24576], P('sp'), may hold values from 0 to 15, never falling along the last dimension, each value on 1 to 3072 neighbouring positions
- sink: float32 [16], P('tp'), may hold values from 3 to 7
- out_weight: bfloat16 [1024, 2048], replicated, may hold values from -0.1875 to 0.1875
- norm_gain_one: float32 [2048], replicated, may hold values from 0.1 to 1.9
- group: int32 [24576], P('sp'), may hold values from 0 to 3, as said below
- member: int32 [24576, 2], P('sp'), may hold values from 0 to 7, as said below
- route_weight: float32 [24576, 2], P('sp'), may hold values from 0.25 to 1
- gate_weight: bfloat16 [32, 2048, 1024], P('sp', None, 'tp'), may hold values from -0.125 to 0.125
- up_weight: bfloat16 [32, 2048, 1024], P('sp', None, 'tp'), may hold values from -0.125 to 0.125
- down_weight: bfloat16 [32, 1024, 2048], P('sp', None, 'tp'), may hold values from -0.1875 to 0.1875
- norm_gain_two: float32 [2048], P('tp'), may hold values from 0.1 to 1.9
Outputs:
- output: bfloat16 [24576, 2048], P('sp', 'tp')
The draws below stay inside these ranges and needn't reach their ends.
Inputs may be any that keep to these rules, and one draw needn't show every extreme that they name: In every aligned block of 96 rows no expert (group * 8 + member) is named by more than 12 rows, and one expert, the same in all blocks of a draw, is named by exactly 12 rows of every block. `member`: the 2 members of a row differ.
All inputs are finite; a program needn't handle non-finite values.
Results may differ from the reference program's by a relative error of at most 0.0059.
Values may be sent and summed in bfloat16 or wider, within the bound.
No kernel may reach another device: no remote copies, remote signals or barrier semaphores. Data moves between devices by JAX's collectives and lax.ppermute only.
A program may use at most 128 MiB of HBM per device.

```python
import math
import jax
import jax.numpy as jnp
import numpy as np
from jax import lax

D = 2048
HEADS = 16
KV_HEADS = 8
HEAD_DIM = 64
HALF = 128
FF = 1024
GROUPS = 4
PER_GROUP = 8
TOP = 2
TOK_DEV = 768
TOKENS = 24576
EXPERTS = 32
BLOCK = 96
CAP = 12
N_SP = 32


def attention_inputs(key):
    parts = jax.random.split(key, 2)
    query_out = jnp.clip(jax.random.normal(parts[0], (TOKENS, HEADS * HEAD_DIM), jnp.float32), -6.0, 6.0)
    key_out = jnp.clip(jax.random.normal(parts[1], (TOKENS, KV_HEADS * HEAD_DIM), jnp.float32), -6.0, 6.0)
    return (query_out, key_out)


def draw_queries(key, part):
    return attention_inputs(jax.random.fold_in(key, 11))[0].astype(jnp.bfloat16)


def draw_keys(key, part):
    return attention_inputs(jax.random.fold_in(key, 11))[1].astype(jnp.bfloat16)


def routing(key):
    blocks = TOKENS // BLOCK
    parts = jax.random.split(key, 6)
    hot_expert = jax.random.randint(parts[0], (), 0, GROUPS * PER_GROUP)
    hot_group = hot_expert // PER_GROUP
    hot_member = hot_expert % PER_GROUP
    scores = jax.random.randint(parts[1], (blocks, BLOCK), 0, 1 << 20) * BLOCK + jnp.arange(BLOCK)[None, :]
    rank = jnp.argsort(jnp.argsort(scores, axis=1, stable=True), axis=1, stable=True).astype(jnp.int32)
    shift_hot = jax.random.randint(parts[2], (blocks, 1), 0, PER_GROUP - 1)
    shift_group = jax.random.randint(parts[3], (blocks, 1), 0, GROUPS - 1)
    offset_table = jax.random.randint(parts[4], (blocks, GROUPS - 1), 0, PER_GROUP)
    gap_table = jax.random.randint(parts[5], (blocks, GROUPS - 1), 0, PER_GROUP - 1)
    is_hot = rank < CAP
    hot_second = (hot_member + 1 + (rank + shift_hot) % (PER_GROUP - 1)) % PER_GROUP
    remainder = jnp.maximum(rank - CAP, 0)
    group_slot = (remainder + shift_group) % (GROUPS - 1)
    other_group = (hot_group + 1 + group_slot) % GROUPS
    cycle_turn = remainder // (GROUPS - 1)
    slot_offset = jnp.take_along_axis(offset_table, group_slot, axis=1)
    slot_gap = jnp.take_along_axis(gap_table, group_slot, axis=1)
    first_member = (cycle_turn + slot_offset) % PER_GROUP
    second_member = (first_member + 1 + slot_gap) % PER_GROUP
    group_out = jnp.where(is_hot, hot_group, other_group).reshape(-1)
    member_one = jnp.where(is_hot, hot_member, first_member).reshape(-1)
    member_two = jnp.where(is_hot, hot_second, second_member).reshape(-1)
    return (group_out.astype(jnp.int32), jnp.stack([member_one, member_two], 1).astype(jnp.int32))


def draw_group(key, part):
    return routing(jax.random.fold_in(key, 23))[0]


def draw_member(key, part):
    return routing(jax.random.fold_in(key, 23))[1]


def levels(own_key, dims, cuts, smallest, largest):
    factor_of = 1.0
    for position, blocks in cuts:
        steps = jax.random.uniform(jax.random.fold_in(jax.random.fold_in(own_key, 6), position), (blocks,), jnp.float32, smallest / len(cuts), largest / len(cuts))
        factor_of = factor_of * jnp.repeat(jnp.exp(steps), dims[position] // blocks).reshape((-1,) + (1,) * (len(dims) - 1 - position))
    return factor_of


def profile(amount, total, limit, slope):
    weights = [(1 << 20) // math.isqrt(grade ** slope) + 1 for grade in range(2, amount + 1)]
    surplus, holding = total - limit - (amount - 1), [1] * (amount - 1)
    while surplus > 0:
        movable = [i for i in range(amount - 1) if holding[i] < limit]
        whole, left = sum([weights[i] for i in movable]), surplus
        for i in movable:
            addition = min(limit - holding[i], max(1, left * weights[i] // whole), surplus)
            holding[i] = holding[i] + addition
            surplus = surplus - addition
    return np.array([limit] + holding)


def ragged_sizes(key, number_of, total, bound, slope):
    if number_of == 2:
        one = jax.random.randint(key, (), max(1, total - bound), min(bound, total - 1) + 1)
        return jnp.stack([one, total - one])
    lengths = jnp.asarray(profile(number_of, total, bound, slope), jnp.int32)
    twos = (number_of - 1) // 2
    giver, receiver = lengths[1:1 + 2 * twos:2], lengths[2:2 + 2 * twos:2]
    room = jnp.minimum(giver - 1, bound - receiver)
    shifted = jax.random.randint(jax.random.fold_in(key, 1), (twos,), 0, 1 << 20) % (room + 1)
    lengths = lengths.at[1:1 + 2 * twos:2].set(giver - shifted).at[2:2 + 2 * twos:2].set(receiver + shifted)
    return lengths[jax.random.permutation(jax.random.fold_in(key, 2), number_of)]


def scatter_about(rng, extent, deviation, most, cuts=(), held_as=jnp.bfloat16):
    factor_of = levels(rng, extent, cuts, -0.22, 0.18) if cuts else 1.0
    entries = jax.random.normal(rng, extent, jnp.float32) * deviation * factor_of
    return jnp.minimum(jnp.maximum(entries, -most), most).astype(held_as)


def setup_inputs(seed: int = 0) -> dict:
    splits = jax.random.split(jax.random.key(seed), 16)
    return {
        "residual": scatter_about(splits[0], (TOKENS, D), 1.0, 6.0, ((0, 32),)),
        "queries": draw_queries(jax.random.fold_in(splits[15], 71), 0),
        "keys": draw_keys(jax.random.fold_in(splits[15], 71), 0),
        "values": scatter_about(splits[3], (TOKENS, KV_HEADS * HEAD_DIM), 6.0, 36.0, ((0, 32), (1, 8))),
        "segments": jnp.searchsorted(jnp.cumsum(ragged_sizes(splits[4], N_SP // 2, TOKENS, 4 * TOK_DEV, 1)), jnp.arange(TOKENS), side="right").astype(jnp.int32),
        "sink": jnp.clip(3.0 + 4.0 * jax.random.uniform(splits[5], (HEADS,), jnp.float32) ** levels(splits[5], (HEADS,), ((0, 8),), -0.2, 0.2), 3.0, 7.0),
        "out_weight": scatter_about(splits[6], (HEADS * HEAD_DIM, D), (HEADS * HEAD_DIM) ** -0.5, 0.1875),
        "norm_gain_one": jnp.clip(1.0 + 0.18 * jax.random.normal(splits[7], (D,), jnp.float32), 0.1, 1.9),
        "group": draw_group(jax.random.fold_in(splits[15], 71), 0),
        "member": draw_member(jax.random.fold_in(splits[15], 71), 0),
        "route_weight": jnp.clip(jnp.exp(math.log(1.0) - 1.3862944 * jax.random.uniform(splits[10], (TOKENS, TOP), jnp.float32) ** levels(splits[10], (TOKENS, TOP), ((0, 32),), -0.2, 0.2)), 0.25, 1.0),
        "gate_weight": scatter_about(splits[11], (EXPERTS, D, FF), D ** -0.5, 0.125, ((0, 32), (2, 8))),
        "up_weight": scatter_about(splits[12], (EXPERTS, D, FF), D ** -0.5, 0.125, ((0, 32), (2, 8))),
        "down_weight": scatter_about(splits[13], (EXPERTS, FF, D), FF ** -0.5, 0.1875, ((0, 32), (2, 8))),
        "norm_gain_two": jnp.clip(1.0 + 0.18 * jax.random.normal(splits[14], (D,), jnp.float32), 0.1, 1.9),
    }


ALPHA = 2.0 ** 0.25
EPS = 1e-05

def layer_norm(summed, norm_gain):
    mean_value = lax.optimization_barrier(jnp.mean(summed, -1, keepdims=True))
    variance = lax.optimization_barrier(jnp.mean(jnp.square(summed - mean_value), -1, keepdims=True))
    return ((summed - mean_value) * lax.rsqrt(variance + EPS) * norm_gain).astype(jnp.bfloat16)

def reference(residual, queries, keys, values, segments, sink, out_weight, norm_gain_one, group, member, route_weight, gate_weight, up_weight, down_weight, norm_gain_two):
    seq_total = queries.shape[0]
    group_size = HEADS // KV_HEADS
    query_block = math.gcd(seq_total, 512)
    key_span = query_block + 2 * HALF
    query_heads = queries.reshape(seq_total, KV_HEADS, group_size, HEAD_DIM)
    key_padded = jnp.pad(keys, ((HALF, HALF), (0, 0))).reshape(seq_total + 2 * HALF, KV_HEADS, HEAD_DIM)
    value_padded = jnp.pad(values, ((HALF, HALF), (0, 0))).reshape(seq_total + 2 * HALF, KV_HEADS, HEAD_DIM)
    seg_padded = jnp.pad(segments, (HALF, HALF), constant_values=-1)
    offsets = jnp.arange(key_span)[None, :] - HALF - jnp.arange(query_block)[:, None]
    in_band = jnp.abs(offsets) <= HALF
    sink_heads = sink.astype(jnp.float32).reshape(KV_HEADS, group_size, 1, 1)

    def attend(number):
        row_low = (number * query_block).astype(jnp.int32)
        query_rows = lax.dynamic_slice_in_dim(query_heads, row_low, query_block, 0)
        key_part = lax.dynamic_slice_in_dim(key_padded, row_low, key_span, 0)
        value_part = lax.dynamic_slice_in_dim(value_padded, row_low, key_span, 0)
        seg_query = lax.dynamic_slice_in_dim(segments, row_low, query_block, 0)
        seg_keys = lax.dynamic_slice_in_dim(seg_padded, row_low, key_span, 0)
        allowed = in_band & (seg_query[:, None] == seg_keys[None, :])
        scores = jnp.einsum('qkgd,ckd->kgqc', query_rows.astype(jnp.float32), key_part.astype(jnp.float32)) * HEAD_DIM ** (-0.5)
        masked = jnp.where(allowed, scores, -1e+30)
        peak = jnp.maximum(lax.optimization_barrier(jnp.max(masked, -1, keepdims=True)), sink_heads)
        raised = jnp.where(allowed, jnp.exp(masked - peak), 0.0)
        denominator = lax.optimization_barrier(jnp.sum(raised, -1, keepdims=True)) + jnp.exp(sink_heads - peak)
        weights = (raised / denominator).astype(jnp.bfloat16)
        attended_part = jnp.einsum('kgqc,ckd->qkgd', weights.astype(jnp.float32), value_part.astype(jnp.float32))
        return attended_part.reshape(query_block, HEADS * HEAD_DIM).astype(jnp.bfloat16)
    attended = lax.map(attend, jnp.arange(seq_total // query_block, dtype=jnp.int32)).reshape(seq_total, HEADS * HEAD_DIM)
    mixed = jnp.dot(attended, out_weight, preferred_element_type=jnp.float32)
    pre_one = ALPHA * residual.astype(jnp.float32) + mixed
    normed = layer_norm(pre_one, norm_gain_one.astype(jnp.float32))
    copies = seq_total * TOP
    flat_expert = (group[:, None] * PER_GROUP + member).reshape(-1).astype(jnp.int32)
    normed_ext = jnp.concatenate([normed, jnp.zeros((1, D), jnp.bfloat16)], 0)
    capacity_all = CAP * (TOKENS // BLOCK)

    def expert_rows(expert):
        copy_index = jnp.nonzero(flat_expert == expert, size=capacity_all, fill_value=copies)[0].astype(jnp.int32)
        taken = normed_ext[copy_index // TOP]
        gate_part = jnp.dot(taken, gate_weight[expert], preferred_element_type=jnp.float32)
        up_part = jnp.dot(taken, up_weight[expert], preferred_element_type=jnp.float32)
        hidden = (jax.nn.silu(gate_part) * up_part).astype(jnp.bfloat16)
        result = jnp.dot(hidden, down_weight[expert], preferred_element_type=jnp.float32).astype(jnp.bfloat16)
        return (copy_index, result)
    indices, results = lax.map(expert_rows, jnp.arange(EXPERTS, dtype=jnp.int32))
    per_copy = jnp.zeros((copies + 1, D), jnp.bfloat16).at[indices.reshape(-1)].set(results.reshape(-1, D))
    per_copy = per_copy[:copies].reshape(seq_total, TOP, D)
    combined = lax.optimization_barrier(jnp.sum(route_weight.astype(jnp.float32)[:, :, None] * per_copy.astype(jnp.float32), 1))
    pre_two = ALPHA * normed.astype(jnp.float32) + combined
    return layer_norm(pre_two, norm_gain_two.astype(jnp.float32))
```

```python
import jax
import jax.numpy as jnp
from jax import lax
from jax.experimental import pallas as pl
from jax.experimental.pallas import tpu as pltpu
from jax.sharding import PartitionSpec as P

HEAD_DIM = 64
HALF = 128
PER_GROUP = 8
ALPHA = 2.0**0.25
EPS = 1e-05
NEG = -1e30
F32 = jnp.float32
BF16 = jnp.bfloat16

ROWS = 768
QB = 128
BLOCKS = ROWS // QB
TP = 8
BLK = ROWS // TP
CAP = 12
MAIN = 8
EXTRA = CAP - MAIN
D = 2048
HALF_D = D // 2
WIDE = D + HALF_D
FF = 1024


def dot(a, b):
    return jnp.dot(a, b, preferred_element_type=F32)


def params(mib=48):
    return pltpu.CompilerParams(vmem_limit_bytes=mib * 1024 * 1024)


def iota(shape, dim):
    return lax.broadcasted_iota(jnp.int32, shape, dim)


def pack_kernel(kt, vt, seg, low, high):
    for out, start, row in ((low, 0, 0), (high, ROWS - HALF, BLOCKS - 1)):
        out[0:64, :] = kt[:, start : start + HALF]
        out[64:128, :] = vt[:, start : start + HALF]
        out[128:144, :] = jnp.broadcast_to(seg[row : row + 1, :].astype(F32), (16, HALF)).astype(BF16)


def attend(q, kt, vt, seg_q, seg_k, sink):
    qs = jnp.concatenate([q[:, :HEAD_DIM], q[:, HEAD_DIM:]], axis=0)
    scores = dot(qs, kt) * HEAD_DIM ** (-0.5)
    col = jnp.transpose(jnp.broadcast_to(seg_q, (QB, QB)))
    row_i = iota((QB, QB), 0)
    col_i = iota((QB, QB), 1)
    parts = []
    for n, band in enumerate((col_i >= row_i, None, col_i <= row_i)):
        same = col == jnp.broadcast_to(seg_k[n], (QB, QB))
        parts.append(same if band is None else jnp.logical_and(same, band))
    allowed = jnp.concatenate(parts, axis=1)
    outs = []
    for h in range(2):
        part = jnp.where(allowed, scores[h * QB : (h + 1) * QB], NEG)
        peak = jnp.maximum(jnp.max(part, -1, keepdims=True), sink[h])
        raised = jnp.where(allowed, jnp.exp(part - peak), 0.0)
        denominator = jnp.sum(raised, -1, keepdims=True) + jnp.exp(sink[h] - peak)
        outs.append((raised / denominator).astype(BF16))
    weights = jnp.concatenate(outs, axis=0)
    got = lax.dot_general(weights, vt, (((1,), (1,)), ((), ())), preferred_element_type=F32)
    return jnp.concatenate([got[:QB], got[QB:]], axis=1).astype(BF16)


def interior_kernel(sink, q, kt, vt, seg, out):
    sinks = [jnp.full((QB, 1), sink[h], F32) for h in range(2)]
    rows = [seg[b : b + 1, :].astype(F32) for b in range(BLOCKS)]
    for b in range(1, BLOCKS - 1):
        lo = (b - 1) * QB
        out[b * QB : (b + 1) * QB, :] = attend(
            q[b * QB : (b + 1) * QB, :],
            kt[:, lo : lo + 3 * QB],
            vt[:, lo : lo + 3 * QB],
            rows[b],
            rows[b - 1 : b + 2],
            sinks,
        )


def edge_kernel(sink, q, kt, vt, seg, before, after, part, out):
    sinks = [jnp.full((QB, 1), sink[h], F32) for h in range(2)]
    rows = [seg[b : b + 1, :].astype(F32) for b in range(BLOCKS)]
    out[QB : ROWS - QB, :] = part[QB : ROWS - QB, :]
    out[:QB, :] = attend(
        q[:QB, :],
        jnp.concatenate([before[0:64, :], kt[:, : 2 * QB]], axis=1),
        jnp.concatenate([before[64:128, :], vt[:, : 2 * QB]], axis=1),
        rows[0],
        [before[128:129, :].astype(F32), rows[0], rows[1]],
        sinks,
    )
    lo = ROWS - QB
    out[lo:, :] = attend(
        q[lo:, :],
        jnp.concatenate([kt[:, lo - QB :], after[0:64, :]], axis=1),
        jnp.concatenate([vt[:, lo - QB :], after[64:128, :]], axis=1),
        rows[BLOCKS - 1],
        [rows[BLOCKS - 2], rows[BLOCKS - 1], after[128:129, :].astype(F32)],
        sinks,
    )


def routing_kernel(ids, weight, rows, cols):
    r0 = iota((BLK, BLK), 0)
    r1 = iota((BLK, BLK), 1)
    eye = r0 == r1

    def column(row):
        return jnp.sum(jnp.where(eye, jnp.broadcast_to(row, (BLK, BLK)), 0.0), axis=1, keepdims=True)

    def place(expert, rank):
        is_main = rank < MAIN - 0.5
        main = jnp.where(is_main, expert * MAIN + rank, -1e6)
        extra = jnp.where(is_main, -1e6, expert * MAIN + (rank - MAIN))
        return main, extra

    id_rows = [ids[k : k + 1, :] for k in range(2)]
    id_cols = [column(row) for row in id_rows]
    row_out, col_out = [], []
    for k in range(2):
        rank_row = jnp.zeros((1, BLK), F32)
        rank_col = jnp.zeros((BLK, 1), F32)
        for other in range(2):
            hit = jnp.logical_and(id_cols[other] == id_rows[k], r0 < r1)
            rank_row += jnp.sum(jnp.where(hit, 1.0, 0.0), axis=0, keepdims=True)
            hit = jnp.logical_and(id_cols[k] == id_rows[other], r1 < r0)
            rank_col += jnp.sum(jnp.where(hit, 1.0, 0.0), axis=1, keepdims=True)
        row_out.append(place(id_rows[k], rank_row))
        col_out.append(place(id_cols[k], rank_col))
    zero_row = jnp.zeros((1, BLK), F32)
    rows[...] = jnp.concatenate(
        [row_out[0][0], row_out[1][0], row_out[0][1], row_out[1][1]] + [zero_row] * 4, axis=0
    )
    lane = iota((BLK, 8), 1)
    table = jnp.zeros((BLK, 8), F32)
    for n, c in enumerate(
        [col_out[0][0], col_out[1][0], col_out[0][1], col_out[1][1]]
        + [column(weight[k : k + 1, :]) for k in range(2)]
    ):
        table = jnp.where(lane == n, c, table)
    cols[...] = table


def project_kernel(place, att, weight, residual, gain, rows, normed_out, sent, acc):
    step = pl.program_id(0)

    @pl.when(step == 0)
    def _():
        acc[...] = ALPHA * residual[...].astype(F32)

    acc[...] += dot(jnp.concatenate([att[0], att[1]], axis=1), weight[...])

    @pl.when(step == pl.num_programs(0) - 1)
    def _():
        summed = acc[...]
        mean_value = jnp.mean(summed, -1, keepdims=True)
        variance = jnp.mean(jnp.square(summed - mean_value), -1, keepdims=True)
        normed = ((summed - mean_value) * lax.rsqrt(variance + EPS) * gain[...]).astype(BF16)
        normed_out[...] = normed
        count = sent.shape[0]
        slot = iota((count, BLK), 0).astype(F32)

        def chosen(first, second, shift):
            hit = jnp.logical_or(
                slot == rows[first : first + 1, :] + shift, slot == rows[second : second + 1, :] + shift
            )
            return jnp.where(hit, 1.0, 0.0).astype(BF16)

        sent[:, :D] = dot(chosen(0, 1, 0.0), normed).astype(BF16)
        sent[:, D:] = (
            dot(chosen(2, 3, 0.0), normed[:, :HALF_D])
            + dot(chosen(2, 3, float(EXTRA)), normed[:, HALF_D:])
        ).astype(BF16)


def expert_kernel(arrived, gate, up, down_low, down_high, out, x, hidden):
    step = pl.program_id(0)
    count = arrived.shape[0]
    extras = count // 2

    def spread(shape, extra_dim, other_dim, shift):
        extra = iota(shape, extra_dim)
        hit = ((extra >> 2) << 3) + (extra & 3) + shift == iota(shape, other_dim)
        return jnp.where(hit, 1.0, 0.0).astype(BF16)

    @pl.when(step == 0)
    def _():
        x[:count, :] = arrived[:, :D]
        for h in range(2):
            x[count:, h * HALF_D : (h + 1) * HALF_D] = dot(
                spread((extras, count), 0, 1, h * EXTRA), arrived[:, D:]
            ).astype(BF16)

    @pl.when(step < 4)
    def _():
        gate_part = dot(x[...], jnp.concatenate([gate[0], gate[1]], axis=1))
        up_part = dot(x[...], jnp.concatenate([up[0], up[1]], axis=1))
        hidden[step] = (jax.nn.silu(gate_part) * up_part).astype(BF16)

    @pl.when(step >= 4)
    def _():
        part = pl.multiple_of((step - 4) * 256, 256)
        extra = jnp.zeros((count, 256), F32)
        for h, down in enumerate((down_low, down_high)):
            got = dot(hidden[0], down[0, 0:256, :])
            for n in range(1, 4):
                got += dot(hidden[n], down[0, n * 256 : (n + 1) * 256, :])
            got = got.astype(BF16)
            out[:, pl.ds(h * HALF_D + part, 256)] = got[:count]
            extra += dot(spread((count, extras), 1, 0, h * EXTRA), got[count:])
        out[:, pl.ds(D + part, 256)] = extra.astype(BF16)


def combine_kernel(returned, normed, cols, out):
    count = returned.shape[0]
    slot = iota((BLK, count), 1).astype(F32)
    combined = [jnp.zeros((BLK, HALF_D), F32) for _ in range(2)]
    for k in range(2):
        main = jnp.where(slot == cols[:, k : k + 1], 1.0, 0.0).astype(BF16)
        weight = cols[:, 4 + k : 5 + k]
        for h in range(2):
            extra = jnp.where(slot == cols[:, 2 + k : 3 + k] + float(h * EXTRA), 1.0, 0.0).astype(BF16)
            got = dot(main, returned[:, h * HALF_D : (h + 1) * HALF_D]) + dot(extra, returned[:, D:])
            combined[h] = combined[h] + weight * got
    summed = ALPHA * normed[...].astype(F32) + jnp.concatenate(combined, axis=1)
    mean_value = jnp.mean(summed, -1, keepdims=True)
    variance = jnp.mean(jnp.square(summed - mean_value), -1, keepdims=True)
    scaled = (summed - mean_value) * lax.rsqrt(variance + EPS)
    width = out.shape[2]
    for n in range(out.shape[0]):
        out[n] = scaled[:, n * width : (n + 1) * width].astype(BF16)


VMEM = pl.BlockSpec(memory_space=pltpu.VMEM)
SMEM = pl.BlockSpec(memory_space=pltpu.SMEM)


def shards(
    residual,
    queries,
    keys,
    values,
    segments,
    sink,
    out_weight,
    norm_gain_one,
    group,
    member,
    route_weight,
    gate_weight,
    up_weight,
    down_weight,
    norm_gain_two,
):
    sp = lax.axis_size("sp")
    place = lax.axis_index("tp")
    gates = lax.all_gather(gate_weight[0], "tp", axis=0)
    ups = lax.all_gather(up_weight[0], "tp", axis=0)
    downs = lax.all_gather(down_weight[0], "tp", axis=0)

    kt = keys.T
    vt = values.T
    seg = (segments + 1).reshape(BLOCKS, QB)
    halo = jax.ShapeDtypeStruct((144, HALF), BF16)
    low, high = pl.pallas_call(
        pack_kernel,
        out_shape=(halo, halo),
        in_specs=[VMEM] * 3,
        out_specs=(VMEM, VMEM),
        compiler_params=params(),
        name="pack",
    )(kt, vt, seg)
    forward = [(i, i + 1) for i in range(sp - 1)]
    before = lax.ppermute(high, "sp", forward)
    after = lax.ppermute(low, "sp", [(t, s) for s, t in forward])

    rows_shape = jax.ShapeDtypeStruct((ROWS, 128), BF16)
    interior = pl.pallas_call(
        interior_kernel,
        out_shape=rows_shape,
        in_specs=[SMEM] + [VMEM] * 4,
        out_specs=VMEM,
        compiler_params=params(),
        name="interior",
    )(sink, queries, kt, vt, seg)

    own = place * BLK
    ids = lax.dynamic_slice(group[None, :] * PER_GROUP + member.T, (0, own), (2, BLK)).astype(F32)
    own_weight = lax.dynamic_slice(route_weight.T, (0, own), (2, BLK))
    rows, cols = pl.pallas_call(
        routing_kernel,
        out_shape=(jax.ShapeDtypeStruct((8, BLK), F32), jax.ShapeDtypeStruct((BLK, 8), F32)),
        in_specs=[VMEM] * 2,
        out_specs=(VMEM, VMEM),
        compiler_params=params(),
        name="routing",
    )(ids, own_weight)

    attended = pl.pallas_call(
        edge_kernel,
        out_shape=rows_shape,
        in_specs=[SMEM] + [VMEM] * 7,
        out_specs=VMEM,
        compiler_params=params(),
        name="edges",
    )(sink, queries, kt, vt, seg, before, after, interior)

    heads = lax.all_to_all(attended.reshape(TP, BLK, 128), "tp", 0, 0, tiled=True)

    slots = sp * MAIN
    normed, sent = pl.pallas_call(
        project_kernel,
        grid_spec=pltpu.PrefetchScalarGridSpec(
            num_scalar_prefetch=1,
            grid=(4,),
            in_specs=[
                pl.BlockSpec((2, BLK, 128), lambda i, p: (i, 0, 0)),
                pl.BlockSpec((256, D), lambda i, p: (i, 0)),
                pl.BlockSpec((BLK, D), lambda i, p: (p[0], 0)),
                pl.BlockSpec((1, D), lambda i, p: (0, 0)),
                pl.BlockSpec((8, BLK), lambda i, p: (0, 0)),
            ],
            out_specs=[
                pl.BlockSpec((BLK, D), lambda i, p: (0, 0)),
                pl.BlockSpec((slots, WIDE), lambda i, p: (0, 0)),
            ],
            scratch_shapes=[pltpu.VMEM((BLK, D), F32)],
        ),
        out_shape=(
            jax.ShapeDtypeStruct((BLK, D), BF16),
            jax.ShapeDtypeStruct((slots, WIDE), BF16),
        ),
        compiler_params=params(),
        name="project",
    )(place.reshape(1), heads, out_weight, residual, norm_gain_one.reshape(1, D), rows)

    arrived = lax.all_to_all(sent.reshape(sp, MAIN, WIDE), "sp", 0, 0, tiled=True)

    produced = pl.pallas_call(
        expert_kernel,
        grid=(8,),
        in_specs=[
            pl.BlockSpec((slots, WIDE), lambda i: (0, 0)),
            pl.BlockSpec((2, D, 128), lambda i: (jnp.minimum(i, 3), 0, 0)),
            pl.BlockSpec((2, D, 128), lambda i: (jnp.minimum(i, 3), 0, 0)),
            pl.BlockSpec((1, FF, 256), lambda i: (jnp.maximum(i - 4, 0), 0, 0)),
            pl.BlockSpec((1, FF, 256), lambda i: (jnp.maximum(i, 4), 0, 0)),
        ],
        out_specs=pl.BlockSpec((slots, WIDE), lambda i: (0, 0)),
        out_shape=jax.ShapeDtypeStruct((slots, WIDE), BF16),
        scratch_shapes=[
            pltpu.VMEM((sp * CAP, D), BF16),
            pltpu.VMEM((4, sp * CAP, 256), BF16),
        ],
        compiler_params=params(),
        name="experts",
    )(arrived.reshape(slots, WIDE), gates, ups, downs, downs)

    returned = lax.all_to_all(produced.reshape(sp, MAIN, WIDE), "sp", 0, 0, tiled=True)

    scaled = pl.pallas_call(
        combine_kernel,
        out_shape=jax.ShapeDtypeStruct((TP, BLK, D // TP), BF16),
        in_specs=[VMEM] * 3,
        out_specs=VMEM,
        compiler_params=params(),
        name="combine",
    )(returned.reshape(slots, WIDE), normed, cols)

    last = lax.all_to_all(scaled, "tp", 0, 0, tiled=True).reshape(ROWS, D // TP)
    return (last.astype(F32) * norm_gain_two).astype(BF16)


def solution(mesh):
    in_specs = (
        P("sp", None),
        P("sp", "tp"),
        P("sp", "tp"),
        P("sp", "tp"),
        P("sp"),
        P("tp"),
        P(),
        P(),
        P("sp"),
        P("sp", None),
        P("sp", None),
        P("sp", None, "tp"),
        P("sp", None, "tp"),
        P("sp", None, "tp"),
        P("tp"),
    )
    out_specs = P("sp", "tp")
    return jax.shard_map(shards, mesh=mesh, in_specs=in_specs, out_specs=out_specs, check_vma=False)
```

```python
import functools

import jax
import jax.numpy as jnp
from jax import lax
from jax.experimental import pallas as pl
from jax.experimental.pallas import tpu as pltpu
from jax.sharding import PartitionSpec as P

HEAD_DIM = 64
HALF = 128
PER_GROUP = 8
ALPHA = 2.0**0.25
EPS = 1e-05
NEG = -1e30
F32 = jnp.float32
BF16 = jnp.bfloat16

ROWS = 768
QB = 128
BLOCKS = ROWS // QB
TP = 8
BLK = ROWS // TP
CAP = 12
MAIN = 8
EXTRA = CAP - MAIN
D = 2048
HALF_D = D // 2
WIDE = D + HALF_D
FF = 1024
SPX = 4
SPZ = 8
FAR = (3, 4, 5)
NEAR = (0, 1, 2, 6, 7)
FAR_SLOTS = len(FAR) * SPX * MAIN
SLOTS = SPX * SPZ * MAIN
PIECE = SPX * MAIN


def dot(a, b):
    return jnp.dot(a, b, preferred_element_type=F32)


def params(mib):
    return pltpu.CompilerParams(vmem_limit_bytes=mib * 1024 * 1024)


def iota(shape, dim):
    return lax.broadcasted_iota(jnp.int32, shape, dim)


VMEM = pl.BlockSpec(memory_space=pltpu.VMEM)
SMEM = pl.BlockSpec(memory_space=pltpu.SMEM)
HBM = pl.BlockSpec(memory_space=pltpu.HBM)


def in_hbm(*arrays):
    return [pltpu.with_memory_space_constraint(a, pltpu.HBM) for a in arrays]


def pack_kernel(q, k, v, s, gate, up, down, low, high, packed, qv, kt, vt, seg, sems):
    moves = [
        (k, kt),
        (v, vt),
        (s, seg),
        (gate.at[0], packed.at[0]),
        (up.at[0], packed.at[1]),
        (down.at[0, :, 0:128], packed.at[2, 0:FF]),
        (down.at[0, :, 128:256], packed.at[2, FF : 2 * FF]),
        (q, qv),
    ]
    copies = [pltpu.make_async_copy(a, b, sems.at[n]) for n, (a, b) in enumerate(moves)]
    for copy in copies:
        copy.start()
    for copy in copies[:3]:
        copy.wait()
    for out, start, row in ((low, 0, 0), (high, ROWS - HALF, BLOCKS - 1)):
        out[0:64, :] = kt[:, start : start + HALF]
        out[64:128, :] = vt[:, start : start + HALF]
        out[128:144, :] = jnp.broadcast_to((seg[row : row + 1, :] + 1).astype(F32), (16, HALF)).astype(BF16)
    for copy in copies[3:]:
        copy.wait()


def attend(q, kt, vt, seg_q, seg_k, sink):
    qs = jnp.concatenate([q[:, :HEAD_DIM], q[:, HEAD_DIM:]], axis=0)
    scores = dot(qs, kt) * HEAD_DIM ** (-0.5)
    col = jnp.transpose(jnp.broadcast_to(seg_q, (QB, QB)))
    row_i = iota((QB, QB), 0)
    col_i = iota((QB, QB), 1)
    parts = []
    for n, band in enumerate((col_i >= row_i, None, col_i <= row_i)):
        same = col == jnp.broadcast_to(seg_k[n], (QB, QB))
        parts.append(same if band is None else jnp.logical_and(same, band))
    allowed = jnp.concatenate(parts, axis=1)
    outs = []
    for h in range(2):
        part = jnp.where(allowed, scores[h * QB : (h + 1) * QB], NEG)
        peak = jnp.maximum(jnp.max(part, -1, keepdims=True), sink[h])
        raised = jnp.where(allowed, jnp.exp(part - peak), 0.0)
        denominator = jnp.sum(raised, -1, keepdims=True) + jnp.exp(sink[h] - peak)
        outs.append((raised / denominator).astype(BF16))
    weights = jnp.concatenate(outs, axis=0)
    got = lax.dot_general(weights, vt, (((1,), (1,)), ((), ())), preferred_element_type=F32)
    return jnp.concatenate([got[:QB], got[QB:]], axis=1).astype(BF16)


def interior_kernel(sink, q, kt, vt, seg, out):
    sinks = [jnp.full((QB, 1), sink[h], F32) for h in range(2)]
    rows = [(seg[b : b + 1, :] + 1).astype(F32) for b in range(BLOCKS)]
    for b in range(1, BLOCKS - 1):
        lo = (b - 1) * QB
        out[b * QB : (b + 1) * QB, :] = attend(
            q[b * QB : (b + 1) * QB, :],
            kt[:, lo : lo + 3 * QB],
            vt[:, lo : lo + 3 * QB],
            rows[b],
            rows[b - 1 : b + 2],
            sinks,
        )


def edge_kernel(sink, q, kt, vt, seg, before, after, part, out):
    sinks = [jnp.full((QB, 1), sink[h], F32) for h in range(2)]
    rows = [(seg[b : b + 1, :] + 1).astype(F32) for b in range(BLOCKS)]
    out[QB : ROWS - QB, :] = part[QB : ROWS - QB, :]
    out[:QB, :] = attend(
        q[:QB, :],
        jnp.concatenate([before[0:64, :], kt[:, : 2 * QB]], axis=1),
        jnp.concatenate([before[64:128, :], vt[:, : 2 * QB]], axis=1),
        rows[0],
        [before[128:129, :].astype(F32), rows[0], rows[1]],
        sinks,
    )
    lo = ROWS - QB
    out[lo:, :] = attend(
        q[lo:, :],
        jnp.concatenate([kt[:, lo - QB :], after[0:64, :]], axis=1),
        jnp.concatenate([vt[:, lo - QB :], after[64:128, :]], axis=1),
        rows[BLOCKS - 1],
        [rows[BLOCKS - 2], rows[BLOCKS - 1], after[128:129, :].astype(F32)],
        sinks,
    )


def routing_kernel(where, group, member, weight, residual, rows, cols, own_out, sem):
    place, z, x = where[0], where[1], where[2]
    start = pl.multiple_of(place * BLK, BLK)
    own_copy = pltpu.make_async_copy(residual.at[pl.ds(start, BLK), :], own_out, sem)
    own_copy.start()
    r0 = iota((BLK, BLK), 0)
    r1 = iota((BLK, BLK), 1)
    eye = r0 == r1
    own = iota((BLK, ROWS), 1) == iota((BLK, ROWS), 0) + place * BLK

    def column(row):
        return jnp.sum(jnp.where(own, jnp.broadcast_to(row, (BLK, ROWS)), 0.0), axis=1, keepdims=True)

    def turned(col):
        return jnp.sum(jnp.where(eye, jnp.broadcast_to(col, (BLK, BLK)), 0.0), axis=0, keepdims=True)

    def base(expert):
        expert = expert.astype(jnp.int32)
        dz = (((expert >> 2) & 7) - z) & 7
        dx = ((expert & 3) - x) & 3
        near_at = jnp.where(dz < FAR[0], dz, dz - len(FAR))
        far = jnp.logical_and(dz >= FAR[0], dz <= FAR[-1])
        at = jnp.where(
            far,
            (dx * len(FAR) + dz - FAR[0]) * MAIN,
            FAR_SLOTS + (dx * len(NEAR) + near_at) * MAIN,
        )
        return at.astype(F32)

    def put(expert, rank):
        is_main = rank < MAIN - 0.5
        start = base(expert)
        main = jnp.where(is_main, start + rank, -1e6)
        extra = jnp.where(is_main, -1e6, start + (rank - MAIN))
        return main, extra

    group_col = column(group[...].astype(F32))
    id_cols = [group_col * PER_GROUP + column(member[k : k + 1, :].astype(F32)) for k in range(2)]
    id_rows = [turned(c) for c in id_cols]
    row_out, col_out = [], []
    for k in range(2):
        rank_row = jnp.zeros((1, BLK), F32)
        rank_col = jnp.zeros((BLK, 1), F32)
        for other in range(2):
            hit = jnp.logical_and(id_cols[other] == id_rows[k], r0 < r1)
            rank_row += jnp.sum(jnp.where(hit, 1.0, 0.0), axis=0, keepdims=True)
            hit = jnp.logical_and(id_cols[k] == id_rows[other], r1 < r0)
            rank_col += jnp.sum(jnp.where(hit, 1.0, 0.0), axis=1, keepdims=True)
        row_out.append(put(id_rows[k], rank_row))
        col_out.append(put(id_cols[k], rank_col))
    zero_row = jnp.zeros((1, BLK), F32)
    rows[...] = jnp.concatenate(
        [row_out[0][0], row_out[1][0], row_out[0][1], row_out[1][1]] + [zero_row] * 4, axis=0
    )
    lane = iota((BLK, 8), 1)
    table = jnp.zeros((BLK, 8), F32)
    for n, c in enumerate(
        [col_out[0][0], col_out[1][0], col_out[0][1], col_out[1][1]]
        + [column(weight[k : k + 1, :]) for k in range(2)]
    ):
        table = jnp.where(lane == n, c, table)
    cols[...] = table
    own_copy.wait()


def project_kernel(att, weight, residual, gain, rows, normed_out, *refs):
    sent, matrix, sems = refs[:-2], refs[-2], refs[-1]
    copies = [
        pltpu.make_async_copy(weight.at[n * 256 : (n + 1) * 256, :], matrix.at[n], sems.at[n]) for n in range(4)
    ]
    for copy in copies:
        copy.start()
    summed = ALPHA * residual[...].astype(F32)
    for n, copy in enumerate(copies):
        copy.wait()
        summed += dot(jnp.concatenate([att[2 * n], att[2 * n + 1]], axis=1), matrix[n])
    mean_value = jnp.mean(summed, -1, keepdims=True)
    variance = jnp.mean(jnp.square(summed - mean_value), -1, keepdims=True)
    normed = ((summed - mean_value) * lax.rsqrt(variance + EPS) * gain[...]).astype(BF16)
    normed_out[...] = normed
    slot = iota((SLOTS, BLK), 0).astype(F32)

    def chosen(first, second, shift):
        hit = jnp.logical_or(
            slot == rows[first : first + 1, :] + shift, slot == rows[second : second + 1, :] + shift
        )
        return jnp.where(hit, 1.0, 0.0).astype(BF16)

    main = dot(chosen(0, 1, 0.0), normed).astype(BF16)
    extra = (
        dot(chosen(2, 3, 0.0), normed[:, :HALF_D])
        + dot(chosen(2, 3, float(EXTRA)), normed[:, HALF_D:])
    ).astype(BF16)
    start = 0
    for out in sent:
        end = start + out.shape[0]
        out[:, :D] = main[start:end]
        out[:, D:] = extra[start:end]
        start = end


def turn_kernel(*refs):
    half = [n for n in range(1, len(refs)) if refs[0].shape[0] == (len(refs) - n) * MAIN][0]
    ins, outs = refs[:half], refs[half:]
    for i, a in enumerate(ins):
        for j, b in enumerate(outs):
            b[i * MAIN : (i + 1) * MAIN, :] = a[j * MAIN : (j + 1) * MAIN, :]


def turn(arrays, count, name):
    shape = jax.ShapeDtypeStruct((len(arrays) * MAIN, WIDE), BF16)
    return pl.pallas_call(
        turn_kernel,
        out_shape=[shape] * count,
        in_specs=[VMEM] * len(arrays),
        out_specs=[VMEM] * count,
        compiler_params=params(8),
        name=name,
    )(*arrays)


def expert_kernel(n, *refs):
    arrived, (gate, up, down_low, down_high) = refs[:n], refs[n : n + 4]
    outs, (x, hidden) = refs[n + 4 : 2 * n + 4], refs[2 * n + 4 :]
    step = pl.program_id(0)
    count = n * PIECE
    extras = count // 2

    def spread(shape, extra_dim, other_dim, shift):
        extra = iota(shape, extra_dim)
        hit = ((extra >> 2) << 3) + (extra & 3) + shift == iota(shape, other_dim)
        return jnp.where(hit, 1.0, 0.0).astype(BF16)

    @pl.when(step == 0)
    def _():
        for i, a in enumerate(arrived):
            x[i * PIECE : (i + 1) * PIECE, :] = a[:, :D]
        packed = jnp.concatenate([a[:, D:] for a in arrived], axis=0)
        for h in range(2):
            x[count:, h * HALF_D : (h + 1) * HALF_D] = dot(
                spread((extras, count), 0, 1, h * EXTRA), packed
            ).astype(BF16)

    @pl.when(step < 4)
    def _():
        gate_part = dot(x[...], jnp.concatenate([gate[0, 0], gate[1, 0]], axis=1))
        up_part = dot(x[...], jnp.concatenate([up[0, 0], up[1, 0]], axis=1))
        hidden[step] = (jax.nn.silu(gate_part) * up_part).astype(BF16)

    @pl.when(step >= 4)
    def _():
        part = pl.multiple_of((step - 4) * 256, 256)
        extra = jnp.zeros((count, 256), F32)
        for h, down in enumerate((down_low, down_high)):
            got = jnp.zeros((count + extras, 256), F32)
            for k in range(4):
                rows = slice(k * 256, (k + 1) * 256)
                high = slice(FF + k * 256, FF + (k + 1) * 256)
                got += dot(hidden[k], jnp.concatenate([down[0, 0, rows, :], down[0, 0, high, :]], axis=1))
            got = got.astype(BF16)
            for i, out in enumerate(outs):
                out[:, pl.ds(h * HALF_D + part, 256)] = got[i * PIECE : (i + 1) * PIECE]
            extra += dot(spread((count, extras), 1, 0, h * EXTRA), got[count:])
        for i, out in enumerate(outs):
            out[:, pl.ds(D + part, 256)] = extra[i * PIECE : (i + 1) * PIECE].astype(BF16)


def experts(arrays, weights, name):
    n = len(arrays)
    piece = jax.ShapeDtypeStruct((PIECE, WIDE), BF16)
    whole = pl.BlockSpec((PIECE, WIDE), lambda i: (0, 0))
    rows = n * SPX * CAP
    return pl.pallas_call(
        functools.partial(expert_kernel, n),
        grid=(8,),
        in_specs=[whole] * n
        + [
            pl.BlockSpec((2, 1, D, 128), lambda i: (jnp.minimum(i, 3), 0, 0, 0)),
            pl.BlockSpec((2, 1, D, 128), lambda i: (jnp.minimum(i, 3), 1, 0, 0)),
            pl.BlockSpec((1, 1, D, 128), lambda i: (jnp.maximum(i - 4, 0), 2, 0, 0)),
            pl.BlockSpec((1, 1, D, 128), lambda i: (jnp.maximum(i, 4), 2, 0, 0)),
        ],
        out_specs=[whole] * n,
        out_shape=[piece] * n,
        scratch_shapes=[pltpu.VMEM((rows, D), BF16), pltpu.VMEM((4, rows, 256), BF16)],
        compiler_params=params(32),
        name=name,
    )(*arrays, *in_hbm(weights) * 4)


def combine_kernel(normed, cols, *refs):
    out = refs[-1]
    returned = jnp.concatenate([a[...] for a in refs[:-1]], axis=0)
    count = SLOTS
    slot = iota((BLK, count), 1).astype(F32)
    combined = [jnp.zeros((BLK, HALF_D), F32) for _ in range(2)]
    for k in range(2):
        main = jnp.where(slot == cols[:, k : k + 1], 1.0, 0.0).astype(BF16)
        weight = cols[:, 4 + k : 5 + k]
        for h in range(2):
            extra = jnp.where(slot == cols[:, 2 + k : 3 + k] + float(h * EXTRA), 1.0, 0.0).astype(BF16)
            got = dot(main, returned[:, h * HALF_D : (h + 1) * HALF_D]) + dot(extra, returned[:, D:])
            combined[h] = combined[h] + weight * got
    summed = ALPHA * normed[...].astype(F32) + jnp.concatenate(combined, axis=1)
    mean_value = jnp.mean(summed, -1, keepdims=True)
    variance = jnp.mean(jnp.square(summed - mean_value), -1, keepdims=True)
    scaled = (summed - mean_value) * lax.rsqrt(variance + EPS)
    width = out.shape[2]
    for n in range(out.shape[0]):
        out[n] = scaled[:, n * width : (n + 1) * width].astype(BF16)


def shards(
    residual,
    queries,
    keys,
    values,
    segments,
    sink,
    out_weight,
    norm_gain_one,
    group,
    member,
    route_weight,
    gate_weight,
    up_weight,
    down_weight,
    norm_gain_two,
):
    place = lax.axis_index("tp")
    sp_place = lax.axis_index("sp")
    kt = keys.T
    vt = values.T
    seg = segments.reshape(BLOCKS, QB)
    halo = jax.ShapeDtypeStruct((144, HALF), BF16)
    packed_shape = pltpu.HBM((3, D, 128), BF16)
    local = [jax.ShapeDtypeStruct(a.shape, a.dtype) for a in (queries, kt, vt, seg)]
    low, high, packed, queries, kt, vt, seg = pl.pallas_call(
        pack_kernel,
        out_shape=(halo, halo, packed_shape, *local),
        in_specs=[HBM] * 7,
        out_specs=(VMEM, VMEM, HBM) + (VMEM,) * 4,
        scratch_shapes=[pltpu.SemaphoreType.DMA((8,))],
        compiler_params=params(8),
        name="pack",
    )(*in_hbm(queries, kt, vt, seg, gate_weight, up_weight, down_weight))
    sp = SPX * SPZ
    forward = [(i, i + 1) for i in range(sp - 1)]
    before = lax.ppermute(high, "sp", forward)
    after = lax.ppermute(low, "sp", [(t, s) for s, t in forward])

    weights = lax.all_gather(packed, "tp", axis=0)

    rows_shape = jax.ShapeDtypeStruct((ROWS, 128), BF16)
    interior = pl.pallas_call(
        interior_kernel,
        out_shape=rows_shape,
        in_specs=[SMEM] + [VMEM] * 4,
        out_specs=VMEM,
        compiler_params=params(8),
        name="interior",
    )(sink, queries, kt, vt, seg)

    where = jnp.stack([place, sp_place >> 2, sp_place & 3]).astype(jnp.int32)
    table = (jax.ShapeDtypeStruct((8, BLK), F32), jax.ShapeDtypeStruct((BLK, 8), F32))
    operands = (group.reshape(1, ROWS), member.T, route_weight.T)
    own_shape = jax.ShapeDtypeStruct((BLK, D), BF16)
    rows, cols, own_residual = pl.pallas_call(
        routing_kernel,
        out_shape=table + (own_shape,),
        in_specs=[SMEM] + [VMEM] * 3 + [HBM],
        out_specs=(VMEM,) * 3,
        scratch_shapes=[pltpu.SemaphoreType.DMA(())],
        compiler_params=params(12),
        name="routing",
    )(where, *operands, *in_hbm(residual))

    operands = (queries, kt, vt, seg, before, after, interior)
    attended = pl.pallas_call(
        edge_kernel,
        out_shape=rows_shape,
        in_specs=[SMEM] + [VMEM] * len(operands),
        out_specs=VMEM,
        compiler_params=params(8),
        name="edges",
    )(sink, *operands)

    heads = lax.all_to_all(attended.reshape(TP, BLK, 128), "tp", 0, 0, tiled=True)

    pieces = [jax.ShapeDtypeStruct((n * MAIN, WIDE), BF16) for n in [len(FAR)] * SPX + [len(NEAR)] * SPX]
    normed_shape = jax.ShapeDtypeStruct((BLK, D), BF16)
    normed, *sent = pl.pallas_call(
        project_kernel,
        out_shape=[normed_shape] + pieces,
        in_specs=[VMEM, HBM] + [VMEM] * 3,
        out_specs=[VMEM] * (1 + len(pieces)),
        scratch_shapes=[pltpu.VMEM((4, 256, D), BF16), pltpu.SemaphoreType.DMA((4,))],
        compiler_params=params(24),
        name="project",
    )(heads, *in_hbm(out_weight), own_residual, norm_gain_one.reshape(1, D), rows)

    def along_x(array, shift):
        if shift == 0:
            return array
        pairs = [(z * SPX + x, z * SPX + (x + shift) % SPX) for z in range(SPZ) for x in range(SPX)]
        return lax.ppermute(array, "sp", pairs)

    def along_z(array, shift):
        if shift == 0:
            return array
        pairs = [(z * SPX + x, (z + shift) % SPZ * SPX + x) for z in range(SPZ) for x in range(SPX)]
        return lax.ppermute(array, "sp", pairs)

    returned = []
    for name, zs, mine in (("far", FAR, sent[:SPX]), ("near", NEAR, sent[SPX:])):
        with jax.named_scope(name):
            mine = [along_x(a, d) for d, a in enumerate(mine)]
            mine = turn(mine, len(zs), "turn_" + name)
            mine = [along_z(a, d) for d, a in zip(zs, mine)]
            mine = experts(mine, weights, "experts_" + name)
            mine = [along_z(a, -d) for d, a in zip(zs, mine)]
            mine = turn(mine, SPX, "back_" + name)
            returned += [along_x(a, -d) for d, a in enumerate(mine)]

    scaled = pl.pallas_call(
        combine_kernel,
        out_shape=jax.ShapeDtypeStruct((TP, BLK, D // TP), BF16),
        in_specs=[VMEM] * (2 + 2 * SPX),
        out_specs=VMEM,
        compiler_params=params(16),
        name="combine",
    )(normed, cols, *returned)

    last = lax.all_to_all(scaled, "tp", 0, 0, tiled=True).reshape(ROWS, D // TP)
    return (last.astype(F32) * norm_gain_two).astype(BF16)


def solution(mesh):
    in_specs = (
        P("sp", None),
        P("sp", "tp"),
        P("sp", "tp"),
        P("sp", "tp"),
        P("sp"),
        P("tp"),
        P(),
        P(),
        P("sp"),
        P("sp", None),
        P("sp", None),
        P("sp", None, "tp"),
        P("sp", None, "tp"),
        P("sp", None, "tp"),
        P("tp"),
    )
    out_specs = P("sp", "tp")
    return jax.shard_map(shards, mesh=mesh, in_specs=in_specs, out_specs=out_specs, check_vma=False)
```

```python
import jax
import jax.numpy as jnp
from jax import lax
from jax.experimental import pallas as pl
from jax.experimental.pallas import tpu as pltpu
from jax.sharding import PartitionSpec as P

HEAD_DIM = 64
HALF = 128
PER_GROUP = 8
ALPHA = 2.0**0.25
EPS = 1e-05
NEG = -1e30
F32 = jnp.float32
BF16 = jnp.bfloat16

ROWS = 768
QB = 128
BLOCKS = ROWS // QB
TP = 8
BLK = ROWS // TP
CAP = 12
D = 2048
HALF_D = D // 2
FF = 1024
SPX = 4
SPZ = 8
GROUP = 8
HALF_CAP = GROUP * CAP // 2
WIDE = D + 128
PICK = 2 * CAP
CHUNK = GROUP * PICK


def dot(a, b):
    return jnp.dot(a, b, preferred_element_type=F32)


def params(mib):
    return pltpu.CompilerParams(vmem_limit_bytes=mib * 1024 * 1024)


def iota(shape, dim):
    return lax.broadcasted_iota(jnp.int32, shape, dim)


VMEM = pl.BlockSpec(memory_space=pltpu.VMEM)
SMEM = pl.BlockSpec(memory_space=pltpu.SMEM)
HBM = pl.BlockSpec(memory_space=pltpu.HBM)


def in_hbm(*arrays):
    return [pltpu.with_memory_space_constraint(a, pltpu.HBM) for a in arrays]


def pack_kernel(q, k, v, s, gate, up, down, low, high, packed, qv, kt, vt, seg, held, sems):
    moves = [
        (k, kt),
        (v, vt),
        (s, seg),
        (gate.at[0], held.at[0]),
        (up.at[0], held.at[1]),
        (down.at[0, :, 0:128], held.at[2, 0:FF]),
        (down.at[0, :, 128:256], held.at[2, FF : 2 * FF]),
        (q, qv),
    ]
    copies = [pltpu.make_async_copy(a, b, sems.at[n]) for n, (a, b) in enumerate(moves)]
    for copy in copies:
        copy.start()
    for copy in copies[:3]:
        copy.wait()
    for out, start, row in ((low, 0, 0), (high, ROWS - HALF, BLOCKS - 1)):
        out[0:64, :] = kt[:, start : start + HALF]
        out[64:128, :] = vt[:, start : start + HALF]
        out[128:144, :] = jnp.broadcast_to((seg[row : row + 1, :] + 1).astype(F32), (16, HALF)).astype(BF16)
    for copy in copies[3:7]:
        copy.wait()
    store = pltpu.make_async_copy(held, packed, sems.at[8])
    store.start()
    store.wait()
    copies[7].wait()


def attend(q, kt, vt, seg_q, seg_k, sink):
    qs = jnp.concatenate([q[:, :HEAD_DIM], q[:, HEAD_DIM:]], axis=0)
    scores = dot(qs, kt) * HEAD_DIM ** (-0.5)
    col = jnp.transpose(jnp.broadcast_to(seg_q, (QB, QB)))
    row_i = iota((QB, QB), 0)
    col_i = iota((QB, QB), 1)
    parts = []
    for n, band in enumerate((col_i >= row_i, None, col_i <= row_i)):
        same = col == jnp.broadcast_to(seg_k[n], (QB, QB))
        parts.append(same if band is None else jnp.logical_and(same, band))
    allowed = jnp.concatenate(parts, axis=1)
    outs = []
    for h in range(2):
        part = jnp.where(allowed, scores[h * QB : (h + 1) * QB], NEG)
        peak = jnp.maximum(jnp.max(part, -1, keepdims=True), sink[h])
        raised = jnp.where(allowed, jnp.exp(part - peak), 0.0)
        denominator = jnp.sum(raised, -1, keepdims=True) + jnp.exp(sink[h] - peak)
        outs.append((raised / denominator).astype(BF16))
    weights = jnp.concatenate(outs, axis=0)
    got = lax.dot_general(weights, vt, (((1,), (1,)), ((), ())), preferred_element_type=F32)
    return jnp.concatenate([got[:QB], got[QB:]], axis=1).astype(BF16)


def interior_kernel(sink, q, kt, vt, seg, out):
    sinks = [jnp.full((QB, 1), sink[h], F32) for h in range(2)]
    rows = [(seg[b : b + 1, :] + 1).astype(F32) for b in range(BLOCKS)]
    for b in range(1, BLOCKS - 1):
        lo = (b - 1) * QB
        out[b * QB : (b + 1) * QB, :] = attend(
            q[b * QB : (b + 1) * QB, :],
            kt[:, lo : lo + 3 * QB],
            vt[:, lo : lo + 3 * QB],
            rows[b],
            rows[b - 1 : b + 2],
            sinks,
        )


def edge_kernel(sink, q, kt, vt, seg, before, after, part, out):
    sinks = [jnp.full((QB, 1), sink[h], F32) for h in range(2)]
    rows = [(seg[b : b + 1, :] + 1).astype(F32) for b in range(BLOCKS)]
    out[QB : ROWS - QB, :] = part[QB : ROWS - QB, :]
    out[:QB, :] = attend(
        q[:QB, :],
        jnp.concatenate([before[0:64, :], kt[:, : 2 * QB]], axis=1),
        jnp.concatenate([before[64:128, :], vt[:, : 2 * QB]], axis=1),
        rows[0],
        [before[128:129, :].astype(F32), rows[0], rows[1]],
        sinks,
    )
    lo = ROWS - QB
    out[lo:, :] = attend(
        q[lo:, :],
        jnp.concatenate([kt[:, lo - QB :], after[0:64, :]], axis=1),
        jnp.concatenate([vt[:, lo - QB :], after[64:128, :]], axis=1),
        rows[BLOCKS - 1],
        [rows[BLOCKS - 2], rows[BLOCKS - 1], after[128:129, :].astype(F32)],
        sinks,
    )


def routing_kernel(where, group, member, weight, residual, rows, cols, table_out, own_out, sem):
    place, z = where[0], where[1]
    start = pl.multiple_of(place * BLK, BLK)
    own_copy = pltpu.make_async_copy(residual.at[pl.ds(start, BLK), :], own_out, sem)
    own_copy.start()
    r0 = iota((BLK, BLK), 0)
    r1 = iota((BLK, BLK), 1)
    eye = r0 == r1
    own = iota((BLK, ROWS), 1) == iota((BLK, ROWS), 0) + place * BLK

    def column(row):
        return jnp.sum(jnp.where(own, jnp.broadcast_to(row, (BLK, ROWS)), 0.0), axis=1, keepdims=True)

    def turned(col):
        return jnp.sum(jnp.where(eye, jnp.broadcast_to(col, (BLK, BLK)), 0.0), axis=0, keepdims=True)

    def before(row, col):
        hit = jnp.logical_and(row == col, r1 < r0)
        return jnp.sum(jnp.where(hit, 1.0, 0.0), axis=1, keepdims=True)

    group_col = column(group[...].astype(F32))
    group_row = turned(group_col)
    away = (group_col.astype(jnp.int32) - (z >> 1)) & 3
    near = jnp.where((z & 1) == 0, 3, 1)
    way = jnp.where(away == 0, 0, jnp.where(away == 2, 3, jnp.where(away == near, 1, 2)))
    where_to = way.astype(F32) * HALF_CAP + before(group_row, group_col)
    cols[...] = jnp.broadcast_to(where_to, (BLK, 128))
    rows[...] = jnp.broadcast_to(turned(where_to), (8, BLK))

    member_cols = [column(member[k : k + 1, :].astype(F32)) for k in range(2)]
    id_cols = [group_col * PER_GROUP + m for m in member_cols]
    id_rows = [turned(c) for c in id_cols]
    entries = []
    for k in range(2):
        rank = before(id_rows[0], id_cols[k]) + before(id_rows[1], id_cols[k])
        entries.append(member_cols[k] * PICK + rank + 1.0)
    for k in range(2):
        rest = column(weight[k : k + 1, :])
        for _ in range(3):
            part = rest.astype(BF16).astype(F32)
            entries.append(part)
            rest = rest - part
    lane = iota((BLK, 128), 1)
    table = jnp.zeros((BLK, 128), F32)
    for n, c in enumerate(entries):
        table = jnp.where(lane == n, c, table)
    table_out[...] = table.astype(BF16)
    own_copy.wait()


def project_kernel(att, weight, residual, gain, rows, table, normed_out, *refs):
    sent, matrix, sems = refs[:-2], refs[-2], refs[-1]
    copies = [
        pltpu.make_async_copy(weight.at[n * 256 : (n + 1) * 256, :], matrix.at[n], sems.at[n]) for n in range(4)
    ]
    for copy in copies:
        copy.start()
    summed = ALPHA * residual[...].astype(F32)
    for n, copy in enumerate(copies):
        copy.wait()
        summed += dot(jnp.concatenate([att[2 * n], att[2 * n + 1]], axis=1), matrix[n])
    mean_value = jnp.mean(summed, -1, keepdims=True)
    variance = jnp.mean(jnp.square(summed - mean_value), -1, keepdims=True)
    normed = ((summed - mean_value) * lax.rsqrt(variance + EPS) * gain[...]).astype(BF16)
    normed_out[...] = normed
    slot = iota((4 * HALF_CAP, BLK), 0).astype(F32)
    chosen = jnp.where(slot == rows[0:1, :], 1.0, 0.0).astype(BF16)
    picked = dot(chosen, normed).astype(BF16)
    tables = dot(chosen, table[...]).astype(BF16)
    for n, out in enumerate(sent):
        out[:, :D] = picked[n * HALF_CAP : (n + 1) * HALF_CAP]
        out[:, D:] = tables[n * HALF_CAP : (n + 1) * HALF_CAP]


def expand_kernel(first, second, out, table_out):
    eye = iota((HALF_CAP, HALF_CAP), 0) == iota((HALF_CAP, HALF_CAP), 1)
    slot = iota((CHUNK, HALF_CAP), 0).astype(F32)
    chosen = []
    for n, a in enumerate((first, second)):
        table = a[:, D:]
        table_out[n * HALF_CAP : (n + 1) * HALF_CAP, :] = table
        hit = None
        for k in range(2):
            col = table[:, k : k + 1].astype(F32)
            row = jnp.sum(jnp.where(eye, jnp.broadcast_to(col, eye.shape), 0.0), axis=0, keepdims=True)
            target = jnp.where(row > 0.5, row - 1.0 + n * CAP, -1.0)
            match = slot == target
            hit = match if hit is None else jnp.logical_or(hit, match)
        chosen.append(jnp.where(hit, 1.0, 0.0).astype(BF16))
    out[...] = (dot(chosen[0], first[:, :D]) + dot(chosen[1], second[:, :D])).astype(BF16)


def expert_kernel(x, weights, out, held, hidden, sems):
    copies = [pltpu.make_async_copy(weights.at[n, 0:2], held.at[n, 0:2], sems.at[n]) for n in range(TP)]
    copies += [pltpu.make_async_copy(weights.at[n, 2], held.at[n, 2], sems.at[TP + n]) for n in range(TP)]
    for copy in copies:
        copy.start()
    for i in range(TP // 2):
        copies[2 * i].wait()
        copies[2 * i + 1].wait()
        pair = (held.at[2 * i], held.at[2 * i + 1])
        gate_part = dot(x[...], jnp.concatenate([w[0] for w in pair], axis=1))
        up_part = dot(x[...], jnp.concatenate([w[1] for w in pair], axis=1))
        hidden[:, i * 256 : (i + 1) * 256] = (jax.nn.silu(gate_part) * up_part).astype(BF16)
    for i in range(TP):
        copies[TP + i].wait()
        down = jnp.concatenate([held[i, 2, :FF, :], held[i, 2, FF:, :]], axis=1)
        out[:, i * 256 : (i + 1) * 256] = dot(hidden[...], down).astype(BF16)


def shrink_kernel(produced, table, first, second):
    count = 2 * HALF_CAP
    slot = iota((count, CHUNK), 1).astype(F32)
    origin = jnp.where(iota((count, 1), 0) >= HALF_CAP, float(CAP), 0.0)
    entries = table[...].astype(F32)
    total = jnp.zeros((count, D), F32)
    for k in range(2):
        col = entries[:, k : k + 1]
        target = jnp.where(col > 0.5, col - 1.0 + origin, -1.0)
        chosen = jnp.where(slot == target, 1.0, 0.0).astype(BF16)
        at = 2 + 3 * k
        weight = (entries[:, at : at + 1] + entries[:, at + 1 : at + 2]) + entries[:, at + 2 : at + 3]
        total += weight * dot(chosen, produced[...])
    first[...] = total[:HALF_CAP].astype(BF16)
    second[...] = total[HALF_CAP:].astype(BF16)


def combine_kernel(normed, cols, own, a, b, c, out):
    slot = iota((BLK, 4 * HALF_CAP), 1).astype(F32)
    chosen = jnp.where(slot == cols[:, 0:1], 1.0, 0.0).astype(BF16)
    stacked = jnp.concatenate([own[...], a[...], b[...], c[...]], axis=0)
    summed = ALPHA * normed[...].astype(F32) + dot(chosen, stacked)
    mean_value = jnp.mean(summed, -1, keepdims=True)
    variance = jnp.mean(jnp.square(summed - mean_value), -1, keepdims=True)
    scaled = (summed - mean_value) * lax.rsqrt(variance + EPS)
    width = out.shape[2]
    for n in range(out.shape[0]):
        out[n] = scaled[:, n * width : (n + 1) * width].astype(BF16)


def kernel(body, name, mib, outs, spaces, *operands, scratch=()):
    return pl.pallas_call(
        body,
        out_shape=outs,
        in_specs=spaces,
        out_specs=[VMEM] * len(outs),
        scratch_shapes=list(scratch),
        compiler_params=params(mib),
        name=name,
    )(*operands)


def shards(
    residual,
    queries,
    keys,
    values,
    segments,
    sink,
    out_weight,
    norm_gain_one,
    group,
    member,
    route_weight,
    gate_weight,
    up_weight,
    down_weight,
    norm_gain_two,
):
    place = lax.axis_index("tp")
    sp_place = lax.axis_index("sp")
    kt = keys.T
    vt = values.T
    seg = segments.reshape(BLOCKS, QB)
    halo = jax.ShapeDtypeStruct((144, HALF), BF16)
    packed_shape = pltpu.HBM((3, D, 128), BF16)
    local = [jax.ShapeDtypeStruct(a.shape, a.dtype) for a in (queries, kt, vt, seg)]
    low, high, packed, queries, kt, vt, seg = pl.pallas_call(
        pack_kernel,
        out_shape=(halo, halo, packed_shape, *local),
        in_specs=[HBM] * 7,
        out_specs=(VMEM, VMEM, HBM) + (VMEM,) * 4,
        scratch_shapes=[pltpu.VMEM((3, D, 128), BF16), pltpu.SemaphoreType.DMA((9,))],
        compiler_params=params(8),
        name="pack",
    )(*in_hbm(queries, kt, vt, seg, gate_weight, up_weight, down_weight))
    sp = SPX * SPZ
    forward = [(i, i + 1) for i in range(sp - 1)]
    before = lax.ppermute(high, "sp", forward)
    after = lax.ppermute(low, "sp", [(t, s) for s, t in forward])

    weights = lax.all_gather(packed, "tp", axis=0)

    rows_shape = jax.ShapeDtypeStruct((ROWS, 128), BF16)
    interior = pl.pallas_call(
        interior_kernel,
        out_shape=rows_shape,
        in_specs=[SMEM] + [VMEM] * 4,
        out_specs=VMEM,
        compiler_params=params(8),
        name="interior",
    )(sink, queries, kt, vt, seg)

    where = jnp.stack([place, sp_place >> 2]).astype(jnp.int32)
    rows, cols, table, own_residual = kernel(
        routing_kernel,
        "routing",
        12,
        (
            jax.ShapeDtypeStruct((8, BLK), F32),
            jax.ShapeDtypeStruct((BLK, 128), F32),
            jax.ShapeDtypeStruct((BLK, 128), BF16),
            jax.ShapeDtypeStruct((BLK, D), BF16),
        ),
        [SMEM] + [VMEM] * 3 + [HBM],
        where,
        group.reshape(1, ROWS),
        member.T,
        route_weight.T,
        *in_hbm(residual),
        scratch=[pltpu.SemaphoreType.DMA(())],
    )

    operands = (queries, kt, vt, seg, before, after, interior)
    attended = pl.pallas_call(
        edge_kernel,
        out_shape=rows_shape,
        in_specs=[SMEM] + [VMEM] * len(operands),
        out_specs=VMEM,
        compiler_params=params(8),
        name="edges",
    )(sink, *operands)

    heads = lax.all_to_all(attended.reshape(TP, BLK, 128), "tp", 0, 0, tiled=True)

    normed, *sent = kernel(
        project_kernel,
        "project",
        24,
        [jax.ShapeDtypeStruct((BLK, D), BF16)] + [jax.ShapeDtypeStruct((HALF_CAP, WIDE), BF16)] * 4,
        [VMEM, HBM] + [VMEM] * 4,
        heads,
        *in_hbm(out_weight),
        own_residual,
        norm_gain_one.reshape(1, D),
        rows,
        table,
        scratch=[pltpu.VMEM((4, 256, D), BF16), pltpu.SemaphoreType.DMA((4,))],
    )

    def along_z(array, even, odd):
        step = (even, odd)
        pairs = [(z * SPX + x, (z + step[z % 2]) % SPZ * SPX + x) for z in range(SPZ) for x in range(SPX)]
        return lax.ppermute(array, "sp", pairs)

    def in_group(array):
        groups = [[g * GROUP + n for n in range(GROUP)] for g in range(sp // GROUP)]
        split = array.reshape(GROUP, PICK, D)
        moved = lax.all_to_all(split, "sp", 0, 0, axis_index_groups=groups, tiled=True)
        return moved.reshape(CHUNK, D)

    near = along_z(sent[1], -1, 1)
    other = along_z(sent[2], 2, -2)
    far = along_z(sent[3], -3, 3)
    back = []
    piece = jax.ShapeDtypeStruct((CHUNK, D), BF16)
    for n, pair in enumerate(((sent[0], near), (other, far))):
        spread, tables = kernel(
            expand_kernel,
            "expand",
            12,
            (piece, jax.ShapeDtypeStruct((2 * HALF_CAP, 128), BF16)),
            [VMEM] * 2,
            *pair,
        )
        arrived = in_group(spread)
        (produced,) = kernel(
            expert_kernel,
            "experts",
            24,
            (piece,),
            [VMEM, HBM],
            arrived,
            *in_hbm(weights),
            scratch=[
                pltpu.VMEM((TP, 3, D, 128), BF16),
                pltpu.VMEM((CHUNK, FF), BF16),
                pltpu.SemaphoreType.DMA((2 * TP,)),
            ],
        )
        back += kernel(
            shrink_kernel,
            "shrink",
            12,
            [jax.ShapeDtypeStruct((HALF_CAP, D), BF16)] * 2,
            [VMEM] * 2,
            in_group(produced),
            tables,
        )

    (scaled,) = kernel(
        combine_kernel,
        "combine",
        16,
        (jax.ShapeDtypeStruct((TP, BLK, D // TP), BF16),),
        [VMEM] * 6,
        normed,
        cols,
        back[0],
        along_z(back[1], -1, 1),
        along_z(back[2], -2, 2),
        along_z(back[3], -3, 3),
    )

    last = lax.all_to_all(scaled, "tp", 0, 0, tiled=True).reshape(ROWS, D // TP)
    return (last.astype(F32) * norm_gain_two).astype(BF16)


def solution(mesh):
    in_specs = (
        P("sp", None),
        P("sp", "tp"),
        P("sp", "tp"),
        P("sp", "tp"),
        P("sp"),
        P("tp"),
        P(),
        P(),
        P("sp"),
        P("sp", None),
        P("sp", None),
        P("sp", None, "tp"),
        P("sp", None, "tp"),
        P("sp", None, "tp"),
        P("tp"),
    )
    out_specs = P("sp", "tp")
    return jax.shard_map(shards, mesh=mesh, in_specs=in_specs, out_specs=out_specs, check_vma=False)
```

```python
import jax
import jax.numpy as jnp
from jax import lax
from jax.experimental import pallas as pl
from jax.experimental.pallas import tpu as pltpu
from jax.sharding import PartitionSpec as P


HEAD_DIM = 64
HALF = 128
PER_GROUP = 8
ALPHA = 2.0**0.25
EPS = 1e-05
NEG = -1e30
F32 = jnp.float32
BF16 = jnp.bfloat16

ROWS = 768
QB = 128
BLOCKS = ROWS // QB
TP = 8
BLK = ROWS // TP
CAP = 12
D = 2048
FF = 1024
SPX = 4
SPZ = 8
GROUP = 8
HALF_CAP = GROUP * CAP // 2
WIDE = D + 128
PICK = 2 * CAP
CHUNK = GROUP * PICK


def dot(a, b):
    return jnp.dot(a, b, preferred_element_type=F32)


def params(mib):
    return pltpu.CompilerParams(vmem_limit_bytes=mib * 1024 * 1024)


def iota(shape, dim):
    return lax.broadcasted_iota(jnp.int32, shape, dim)


VMEM = pl.BlockSpec(memory_space=pltpu.VMEM)
SMEM = pl.BlockSpec(memory_space=pltpu.SMEM)
HBM = pl.BlockSpec(memory_space=pltpu.HBM)


def in_hbm(*arrays):
    return [pltpu.with_memory_space_constraint(a, pltpu.HBM) for a in arrays]


def pack_kernel(q, k, v, s, gate, up, down, low, high, head, tail, qv, kt, vt, seg, held, sems):
    moves = [
        (k, kt),
        (v, vt),
        (s, seg),
        (gate.at[0], held.at[0, 0:D]),
        (up.at[0, 0:FF], held.at[0, D : D + FF]),
        (up.at[0, FF:D], held.at[1, 0:FF]),
        (down.at[0, :, 0:128], held.at[1, FF:D]),
        (down.at[0, :, 128:256], held.at[1, D : D + FF]),
        (q, qv),
    ]
    copies = [pltpu.make_async_copy(a, b, sems.at[n]) for n, (a, b) in enumerate(moves)]
    for copy in copies:
        copy.start()
    for copy in copies[:3]:
        copy.wait()
    for out, start, row in ((low, 0, 0), (high, ROWS - HALF, BLOCKS - 1)):
        out[0:64, :] = kt[:, start : start + HALF]
        out[64:128, :] = vt[:, start : start + HALF]
        out[128:144, :] = jnp.broadcast_to((seg[row : row + 1, :] + 1).astype(F32), (16, HALF)).astype(BF16)
    for copy in copies[3:8]:
        copy.wait()
    stores = [pltpu.make_async_copy(held.at[n], out, sems.at[9 + n]) for n, out in enumerate((head, tail))]
    for store in stores:
        store.start()
    for store in stores:
        store.wait()
    copies[8].wait()


def attend(q, kt, vt, seg_q, seg_k, sink):
    qs = jnp.concatenate([q[:, :HEAD_DIM], q[:, HEAD_DIM:]], axis=0)
    scores = dot(qs, kt) * HEAD_DIM ** (-0.5)
    col = jnp.transpose(jnp.broadcast_to(seg_q, (QB, QB)))
    row_i = iota((QB, QB), 0)
    col_i = iota((QB, QB), 1)
    parts = []
    for n, band in enumerate((col_i >= row_i, None, col_i <= row_i)):
        same = col == jnp.broadcast_to(seg_k[n], (QB, QB))
        parts.append(same if band is None else jnp.logical_and(same, band))
    allowed = jnp.concatenate(parts, axis=1)
    outs = []
    for h in range(2):
        part = jnp.where(allowed, scores[h * QB : (h + 1) * QB], NEG)
        peak = jnp.maximum(jnp.max(part, -1, keepdims=True), sink[h])
        raised = jnp.where(allowed, jnp.exp(part - peak), 0.0)
        denominator = jnp.sum(raised, -1, keepdims=True) + jnp.exp(sink[h] - peak)
        outs.append((raised / denominator).astype(BF16))
    weights = jnp.concatenate(outs, axis=0)
    got = lax.dot_general(weights, vt, (((1,), (1,)), ((), ())), preferred_element_type=F32)
    return jnp.concatenate([got[:QB], got[QB:]], axis=1).astype(BF16)


def interior_kernel(sink, q, kt, vt, seg, out):
    sinks = [jnp.full((QB, 1), sink[h], F32) for h in range(2)]
    rows = [(seg[b : b + 1, :] + 1).astype(F32) for b in range(BLOCKS)]
    for b in range(1, BLOCKS - 1):
        lo = (b - 1) * QB
        out[b * QB : (b + 1) * QB, :] = attend(
            q[b * QB : (b + 1) * QB, :],
            kt[:, lo : lo + 3 * QB],
            vt[:, lo : lo + 3 * QB],
            rows[b],
            rows[b - 1 : b + 2],
            sinks,
        )


def edge_kernel(sink, q, kt, vt, seg, before, after, part, out):
    sinks = [jnp.full((QB, 1), sink[h], F32) for h in range(2)]
    rows = [(seg[b : b + 1, :] + 1).astype(F32) for b in range(BLOCKS)]
    out[QB : ROWS - QB, :] = part[QB : ROWS - QB, :]
    out[:QB, :] = attend(
        q[:QB, :],
        jnp.concatenate([before[0:64, :], kt[:, : 2 * QB]], axis=1),
        jnp.concatenate([before[64:128, :], vt[:, : 2 * QB]], axis=1),
        rows[0],
        [before[128:129, :].astype(F32), rows[0], rows[1]],
        sinks,
    )
    lo = ROWS - QB
    out[lo:, :] = attend(
        q[lo:, :],
        jnp.concatenate([kt[:, lo - QB :], after[0:64, :]], axis=1),
        jnp.concatenate([vt[:, lo - QB :], after[64:128, :]], axis=1),
        rows[BLOCKS - 1],
        [rows[BLOCKS - 2], rows[BLOCKS - 1], after[128:129, :].astype(F32)],
        sinks,
    )


def routing_kernel(where, group, member, weight, residual, rows, cols, table_out, own_out, sem):
    place, z = where[0], where[1]
    start = pl.multiple_of(place * BLK, BLK)
    own_copy = pltpu.make_async_copy(residual.at[pl.ds(start, BLK), :], own_out, sem)
    own_copy.start()
    r0 = iota((BLK, BLK), 0)
    r1 = iota((BLK, BLK), 1)
    eye = r0 == r1
    own = iota((BLK, ROWS), 1) == iota((BLK, ROWS), 0) + place * BLK

    def column(row):
        return jnp.sum(jnp.where(own, jnp.broadcast_to(row, (BLK, ROWS)), 0.0), axis=1, keepdims=True)

    def turned(col):
        return jnp.sum(jnp.where(eye, jnp.broadcast_to(col, (BLK, BLK)), 0.0), axis=0, keepdims=True)

    def before(row, col):
        hit = jnp.logical_and(row == col, r1 < r0)
        return jnp.sum(jnp.where(hit, 1.0, 0.0), axis=1, keepdims=True)

    group_col = column(group[...].astype(F32))
    group_row = turned(group_col)
    away = (group_col.astype(jnp.int32) - (z >> 1)) & 3
    near = jnp.where((z & 1) == 0, 3, 1)
    way = jnp.where(away == 0, 0, jnp.where(away == 2, 3, jnp.where(away == near, 1, 2)))
    where_to = way.astype(F32) * HALF_CAP + before(group_row, group_col)
    cols[...] = jnp.broadcast_to(where_to, (BLK, 128))
    rows[...] = jnp.broadcast_to(turned(where_to), (8, BLK))

    member_cols = [column(member[k : k + 1, :].astype(F32)) for k in range(2)]
    id_cols = [group_col * PER_GROUP + m for m in member_cols]
    id_rows = [turned(c) for c in id_cols]
    entries = []
    for k in range(2):
        rank = before(id_rows[0], id_cols[k]) + before(id_rows[1], id_cols[k])
        entries.append(member_cols[k] * PICK + rank + 1.0)
    for k in range(2):
        rest = column(weight[k : k + 1, :])
        for _ in range(3):
            part = rest.astype(BF16).astype(F32)
            entries.append(part)
            rest = rest - part
    lane = iota((BLK, 128), 1)
    table = jnp.zeros((BLK, 128), F32)
    for n, c in enumerate(entries):
        table = jnp.where(lane == n, c, table)
    table_out[...] = table.astype(BF16)
    own_copy.wait()


def project_kernel(att, weight, residual, gain, rows, table, normed_out, *refs):
    sent, matrix, sems = refs[:-2], refs[-2], refs[-1]
    copies = [
        pltpu.make_async_copy(weight.at[n * 256 : (n + 1) * 256, :], matrix.at[n], sems.at[n]) for n in range(4)
    ]
    for copy in copies:
        copy.start()
    summed = ALPHA * residual[...].astype(F32)
    for n, copy in enumerate(copies):
        copy.wait()
        summed += dot(jnp.concatenate([att[2 * n], att[2 * n + 1]], axis=1), matrix[n])
    mean_value = jnp.mean(summed, -1, keepdims=True)
    variance = jnp.mean(jnp.square(summed - mean_value), -1, keepdims=True)
    normed = ((summed - mean_value) * lax.rsqrt(variance + EPS) * gain[...]).astype(BF16)
    normed_out[...] = normed
    slot = iota((4 * HALF_CAP, BLK), 0).astype(F32)
    chosen = jnp.where(slot == rows[0:1, :], 1.0, 0.0).astype(BF16)
    picked = dot(chosen, normed).astype(BF16)
    tables = dot(chosen, table[...]).astype(BF16)
    for n, out in enumerate(sent):
        out[:, :D] = picked[n * HALF_CAP : (n + 1) * HALF_CAP]
        out[:, D:] = tables[n * HALF_CAP : (n + 1) * HALF_CAP]


def expand_kernel(first, second, out, table_out):
    eye = iota((HALF_CAP, HALF_CAP), 0) == iota((HALF_CAP, HALF_CAP), 1)
    slot = iota((CHUNK, HALF_CAP), 0).astype(F32)
    chosen = []
    for n, a in enumerate((first, second)):
        table = a[:, D:]
        table_out[n * HALF_CAP : (n + 1) * HALF_CAP, :] = table
        hit = None
        for k in range(2):
            col = table[:, k : k + 1].astype(F32)
            row = jnp.sum(jnp.where(eye, jnp.broadcast_to(col, eye.shape), 0.0), axis=0, keepdims=True)
            target = jnp.where(row > 0.5, row - 1.0 + n * CAP, -1.0)
            match = slot == target
            hit = match if hit is None else jnp.logical_or(hit, match)
        chosen.append(jnp.where(hit, 1.0, 0.0).astype(BF16))
    out[...] = (dot(chosen[0], first[:, :D]) + dot(chosen[1], second[:, :D])).astype(BF16)


def expert_kernel(order, x, *refs):
    weights, (out, gate, up, down, hidden, sems) = refs[: 2 * TP], refs[2 * TP :]
    moves = []
    for n in range(TP):
        head, tail = weights[2 * n], weights[2 * n + 1]
        moves.append((head.at[0:D, :], gate.at[n]))
        moves.append((head.at[D:, :], up.at[n, 0:FF]))
        moves.append((tail.at[0:FF, :], up.at[n, FF:D]))
    for n in range(TP):
        moves.append((weights[2 * n + 1].at[FF:, :], down.at[n]))
    copies = [pltpu.make_async_copy(a, b, sems.at[n]) for n, (a, b) in enumerate(moves)]
    for copy in copies:
        copy.start()
    for n in range(TP):
        for copy in copies[3 * n : 3 * n + 3]:
            copy.wait()
        both = dot(x[...], jnp.concatenate([gate[n], up[n]], axis=1))
        hidden[order[n]] = (jax.nn.silu(both[:, :128]) * both[:, 128:]).astype(BF16)
    units = jnp.concatenate([hidden[n] for n in range(TP)], axis=1)
    for n in range(TP):
        copies[3 * TP + n].wait()
        columns = jnp.concatenate([down[n, :FF, :], down[n, FF:, :]], axis=1)
        out[:, pl.ds(pl.multiple_of(order[n] * 256, 256), 256)] = dot(units, columns).astype(BF16)


def shrink_kernel(produced, table, first, second):
    count = 2 * HALF_CAP
    slot = iota((count, CHUNK), 1).astype(F32)
    origin = jnp.where(iota((count, 1), 0) >= HALF_CAP, float(CAP), 0.0)
    entries = table[...].astype(F32)
    total = jnp.zeros((count, D), F32)
    for k in range(2):
        col = entries[:, k : k + 1]
        target = jnp.where(col > 0.5, col - 1.0 + origin, -1.0)
        chosen = jnp.where(slot == target, 1.0, 0.0).astype(BF16)
        at = 2 + 3 * k
        weight = (entries[:, at : at + 1] + entries[:, at + 1 : at + 2]) + entries[:, at + 2 : at + 3]
        total += weight * dot(chosen, produced[...])
    first[...] = total[:HALF_CAP].astype(BF16)
    second[...] = total[HALF_CAP:].astype(BF16)


def combine_kernel(normed, cols, own, a, b, c, out):
    slot = iota((BLK, 4 * HALF_CAP), 1).astype(F32)
    chosen = jnp.where(slot == cols[:, 0:1], 1.0, 0.0).astype(BF16)
    stacked = jnp.concatenate([own[...], a[...], b[...], c[...]], axis=0)
    summed = ALPHA * normed[...].astype(F32) + dot(chosen, stacked)
    mean_value = jnp.mean(summed, -1, keepdims=True)
    variance = jnp.mean(jnp.square(summed - mean_value), -1, keepdims=True)
    scaled = (summed - mean_value) * lax.rsqrt(variance + EPS)
    width = out.shape[2]
    for n in range(out.shape[0]):
        out[n] = scaled[:, n * width : (n + 1) * width].astype(BF16)


def kernel(body, mib, outs, spaces, *operands, scratch=()):
    return pl.pallas_call(
        body,
        out_shape=outs,
        in_specs=spaces,
        out_specs=[VMEM] * len(outs),
        scratch_shapes=list(scratch),
        compiler_params=params(mib),
    )(*operands)


def layer(
    residual,
    queries,
    keys,
    values,
    segments,
    sink,
    out_weight,
    norm_gain_one,
    group,
    member,
    route_weight,
    gate_weight,
    up_weight,
    down_weight,
    norm_gain_two,
):
    place = lax.axis_index("tp")
    sp_place = lax.axis_index("sp")
    kt = keys.T
    vt = values.T
    seg = segments.reshape(BLOCKS, QB)
    halo = jax.ShapeDtypeStruct((144, HALF), BF16)
    packed_shape = pltpu.HBM((D + FF, 128), BF16)
    local = [jax.ShapeDtypeStruct(a.shape, a.dtype) for a in (queries, kt, vt, seg)]
    low, high, head, tail, queries, kt, vt, seg = pl.pallas_call(
        pack_kernel,
        out_shape=(halo, halo, packed_shape, packed_shape, *local),
        in_specs=[HBM] * 7,
        out_specs=(VMEM, VMEM, HBM, HBM) + (VMEM,) * 4,
        scratch_shapes=[pltpu.VMEM((2, D + FF, 128), BF16), pltpu.SemaphoreType.DMA((11,))],
        compiler_params=params(8),
        name="pack",
    )(*in_hbm(queries, kt, vt, seg, gate_weight, up_weight, down_weight))
    sp = SPX * SPZ
    forward = [(i, i + 1) for i in range(sp - 1)]
    before = lax.ppermute(high, "sp", forward)
    after = lax.ppermute(low, "sp", [(t, s) for s, t in forward])

    def along_y(array, shift):
        pairs = [(y * 2 + c, (y + shift) % 4 * 2 + c) for y in range(4) for c in range(2)]
        return lax.ppermute(array, "tp", pairs)

    def swapped(array):
        return lax.ppermute(array, "tp", [(n, n ^ 1) for n in range(TP)])

    from_low, from_high = along_y(head, 1), along_y(head, -1)
    tail_low, tail_high = along_y(tail, 1), along_y(tail, -1)
    head_far = along_y(from_low, 1)
    tail_far = along_y(tail_high, -1)
    other_heads = [swapped(a) for a in (head, from_low, from_high)]
    other_tails = [swapped(a) for a in (tail, tail_low, tail_high)]
    other_heads.append(swapped(head_far))
    other_tails.append(swapped(tail_far))
    heads_all = [head, from_low, from_high, head_far] + other_heads
    tails_all = [tail, tail_low, tail_high, tail_far] + other_tails
    weights = [a for pair in zip(heads_all, tails_all) for a in pair]

    rows_shape = jax.ShapeDtypeStruct((ROWS, 128), BF16)
    interior = pl.pallas_call(
        interior_kernel,
        out_shape=rows_shape,
        in_specs=[SMEM] + [VMEM] * 4,
        out_specs=VMEM,
        compiler_params=params(8),
        name="interior",
    )(sink, queries, kt, vt, seg)

    where = jnp.stack([place, sp_place >> 2]).astype(jnp.int32)
    rows, cols, table, own_residual = kernel(
        routing_kernel,
        12,
        (
            jax.ShapeDtypeStruct((8, BLK), F32),
            jax.ShapeDtypeStruct((BLK, 128), F32),
            jax.ShapeDtypeStruct((BLK, 128), BF16),
            jax.ShapeDtypeStruct((BLK, D), BF16),
        ),
        [SMEM] + [VMEM] * 3 + [HBM],
        where,
        group.reshape(1, ROWS),
        member.T,
        route_weight.T,
        *in_hbm(residual),
        scratch=[pltpu.SemaphoreType.DMA(())],
    )

    operands = (queries, kt, vt, seg, before, after, interior)
    attended = pl.pallas_call(
        edge_kernel,
        out_shape=rows_shape,
        in_specs=[SMEM] + [VMEM] * len(operands),
        out_specs=VMEM,
        compiler_params=params(8),
        name="edges",
    )(sink, *operands)

    heads = lax.all_to_all(attended.reshape(TP, BLK, 128), "tp", 0, 0, tiled=True)

    normed, *sent = kernel(
        project_kernel,
        24,
        [jax.ShapeDtypeStruct((BLK, D), BF16)] + [jax.ShapeDtypeStruct((HALF_CAP, WIDE), BF16)] * 4,
        [VMEM, HBM] + [VMEM] * 4,
        heads,
        *in_hbm(out_weight),
        own_residual,
        norm_gain_one.reshape(1, D),
        rows,
        table,
        scratch=[pltpu.VMEM((4, 256, D), BF16), pltpu.SemaphoreType.DMA((4,))],
    )

    def along_z(array, even, odd):
        step = (even, odd)
        pairs = [(z * SPX + x, (z + step[z % 2]) % SPZ * SPX + x) for z in range(SPZ) for x in range(SPX)]
        return lax.ppermute(array, "sp", pairs)

    def in_group(array):
        groups = [[g * GROUP + n for n in range(GROUP)] for g in range(sp // GROUP)]
        split = array.reshape(GROUP, PICK, D)
        moved = lax.all_to_all(split, "sp", 0, 0, axis_index_groups=groups, tiled=True)
        return moved.reshape(CHUNK, D)

    piece = jax.ShapeDtypeStruct((CHUNK, D), BF16)

    def spread(first, second):
        out = (piece, jax.ShapeDtypeStruct((2 * HALF_CAP, 128), BF16))
        rows, tables = kernel(expand_kernel, 12, out, [VMEM] * 2, first, second)
        return in_group(rows), tables

    def shrink(produced, tables):
        out = [jax.ShapeDtypeStruct((HALF_CAP, D), BF16)] * 2
        return kernel(shrink_kernel, 12, out, [VMEM] * 2, in_group(produced), tables)

    near = along_z(sent[1], -1, 1)
    other = along_z(sent[2], 2, -2)
    far = along_z(sent[3], -3, 3)
    rows_one, tables_one = spread(sent[0], near)
    rows_two, tables_two = spread(other, far)

    away = jnp.array([0, -2, 2, 4], jnp.int32)
    order = (jnp.concatenate([place + away, (place ^ 1) + away]) & 7).astype(jnp.int32)

    def apply(rows):
        return kernel(
            expert_kernel,
            24,
            (piece,),
            [SMEM, VMEM] + [HBM] * (2 * TP),
            order,
            rows,
            *in_hbm(*weights),
            scratch=[
                pltpu.VMEM((TP, D, 128), BF16),
                pltpu.VMEM((TP, D, 128), BF16),
                pltpu.VMEM((TP, D, 128), BF16),
                pltpu.VMEM((TP, CHUNK, 128), BF16),
                pltpu.SemaphoreType.DMA((4 * TP,)),
            ],
        )[0]

    made_one = apply(rows_one)
    made_two = apply(rows_two)
    back_two = shrink(made_two, tables_two)
    back_one = shrink(made_one, tables_one)
    back = [*back_one, *back_two]

    (scaled,) = kernel(
        combine_kernel,
        16,
        (jax.ShapeDtypeStruct((TP, BLK, D // TP), BF16),),
        [VMEM] * 6,
        normed,
        cols,
        back[0],
        along_z(back[1], -1, 1),
        along_z(back[2], -2, 2),
        along_z(back[3], -3, 3),
    )

    last = lax.all_to_all(scaled, "tp", 0, 0, tiled=True).reshape(ROWS, D // TP)
    return (last.astype(F32) * norm_gain_two).astype(BF16)


def solution(mesh):
    in_specs = (
        P("sp", None),
        P("sp", "tp"),
        P("sp", "tp"),
        P("sp", "tp"),
        P("sp"),
        P("tp"),
        P(),
        P(),
        P("sp"),
        P("sp", None),
        P("sp", None),
        P("sp", None, "tp"),
        P("sp", None, "tp"),
        P("sp", None, "tp"),
        P("tp"),
    )
    out_specs = P("sp", "tp")
    return jax.shard_map(layer, mesh=mesh, in_specs=in_specs, out_specs=out_specs, check_vma=False)
```

```python
import jax
import jax.numpy as jnp
from jax import lax
from jax.experimental import pallas as pl
from jax.experimental.pallas import tpu as pltpu
from jax.sharding import PartitionSpec as P


HEAD_DIM = 64
HALF = 128
PER_GROUP = 8
ALPHA = 2.0**0.25
EPS = 1e-05
NEG = -1e30
F32 = jnp.float32
BF16 = jnp.bfloat16

ROWS = 768
QB = 128
BLOCKS = ROWS // QB
TP = 8
BLK = ROWS // TP
CAP = 12
D = 2048
FF = 1024
SPX = 4
SPZ = 8
GROUP = 8
HALF_CAP = GROUP * CAP // 2
WIDE = D + 128
PICK = 2 * CAP
CHUNK = GROUP * PICK


def dot(a, b):
    return jnp.dot(a, b, preferred_element_type=F32)


def params(mib):
    return pltpu.CompilerParams(vmem_limit_bytes=mib * 1024 * 1024)


def iota(shape, dim):
    return lax.broadcasted_iota(jnp.int32, shape, dim)


VMEM = pl.BlockSpec(memory_space=pltpu.VMEM)
SMEM = pl.BlockSpec(memory_space=pltpu.SMEM)
HBM = pl.BlockSpec(memory_space=pltpu.HBM)


def in_hbm(*arrays):
    return [pltpu.with_memory_space_constraint(a, pltpu.HBM) for a in arrays]


def pack_kernel(q, k, v, s, gate, up, down, low, high, head, tail, qv, kt, vt, seg, held, sems):
    moves = [
        (k, kt),
        (v, vt),
        (s, seg),
        (gate.at[0], held.at[0, 0:D]),
        (up.at[0, 0:FF], held.at[0, D : D + FF]),
        (up.at[0, FF:D], held.at[1, 0:FF]),
        (down.at[0, :, 0:128], held.at[1, FF:D]),
        (down.at[0, :, 128:256], held.at[1, D : D + FF]),
        (q, qv),
    ]
    copies = [pltpu.make_async_copy(a, b, sems.at[n]) for n, (a, b) in enumerate(moves)]
    for copy in copies:
        copy.start()
    for copy in copies[:3]:
        copy.wait()
    for out, start, row in ((low, 0, 0), (high, ROWS - HALF, BLOCKS - 1)):
        out[0:64, :] = kt[:, start : start + HALF]
        out[64:128, :] = vt[:, start : start + HALF]
        out[128:144, :] = jnp.broadcast_to((seg[row : row + 1, :] + 1).astype(F32), (16, HALF)).astype(BF16)
    for copy in copies[3:8]:
        copy.wait()
    stores = [pltpu.make_async_copy(held.at[n], out, sems.at[9 + n]) for n, out in enumerate((head, tail))]
    for store in stores:
        store.start()
    for store in stores:
        store.wait()
    copies[8].wait()


def attend(q, kt, vt, seg_q, seg_k, sink):
    qs = jnp.concatenate([q[:, :HEAD_DIM], q[:, HEAD_DIM:]], axis=0)
    scores = dot(qs, kt) * HEAD_DIM ** (-0.5)
    col = jnp.transpose(jnp.broadcast_to(seg_q, (QB, QB)))
    row_i = iota((QB, QB), 0)
    col_i = iota((QB, QB), 1)
    parts = []
    for n, band in enumerate((col_i >= row_i, None, col_i <= row_i)):
        same = col == jnp.broadcast_to(seg_k[n], (QB, QB))
        parts.append(same if band is None else jnp.logical_and(same, band))
    allowed = jnp.concatenate(parts, axis=1)
    outs = []
    for h in range(2):
        part = jnp.where(allowed, scores[h * QB : (h + 1) * QB], NEG)
        peak = jnp.maximum(jnp.max(part, -1, keepdims=True), sink[h])
        raised = jnp.where(allowed, jnp.exp(part - peak), 0.0)
        denominator = jnp.sum(raised, -1, keepdims=True) + jnp.exp(sink[h] - peak)
        outs.append((raised / denominator).astype(BF16))
    weights = jnp.concatenate(outs, axis=0)
    got = lax.dot_general(weights, vt, (((1,), (1,)), ((), ())), preferred_element_type=F32)
    return jnp.concatenate([got[:QB], got[QB:]], axis=1).astype(BF16)


def interior_kernel(sink, q, kt, vt, seg, out):
    sinks = [jnp.full((QB, 1), sink[h], F32) for h in range(2)]
    rows = [(seg[b : b + 1, :] + 1).astype(F32) for b in range(BLOCKS)]
    for b in range(1, BLOCKS - 1):
        lo = (b - 1) * QB
        out[b * QB : (b + 1) * QB, :] = attend(
            q[b * QB : (b + 1) * QB, :],
            kt[:, lo : lo + 3 * QB],
            vt[:, lo : lo + 3 * QB],
            rows[b],
            rows[b - 1 : b + 2],
            sinks,
        )


def edge_kernel(sink, q, kt, vt, seg, before, after, part, out):
    sinks = [jnp.full((QB, 1), sink[h], F32) for h in range(2)]
    rows = [(seg[b : b + 1, :] + 1).astype(F32) for b in range(BLOCKS)]
    out[QB : ROWS - QB, :] = part[QB : ROWS - QB, :]
    out[:QB, :] = attend(
        q[:QB, :],
        jnp.concatenate([before[0:64, :], kt[:, : 2 * QB]], axis=1),
        jnp.concatenate([before[64:128, :], vt[:, : 2 * QB]], axis=1),
        rows[0],
        [before[128:129, :].astype(F32), rows[0], rows[1]],
        sinks,
    )
    lo = ROWS - QB
    out[lo:, :] = attend(
        q[lo:, :],
        jnp.concatenate([kt[:, lo - QB :], after[0:64, :]], axis=1),
        jnp.concatenate([vt[:, lo - QB :], after[64:128, :]], axis=1),
        rows[BLOCKS - 1],
        [rows[BLOCKS - 2], rows[BLOCKS - 1], after[128:129, :].astype(F32)],
        sinks,
    )


def routing_kernel(where, group, member, weight, residual, rows, cols, table_out, own_out, sem):
    place, z = where[0], where[1]
    start = pl.multiple_of(place * BLK, BLK)
    own_copy = pltpu.make_async_copy(residual.at[pl.ds(start, BLK), :], own_out, sem)
    own_copy.start()
    r0 = iota((BLK, BLK), 0)
    r1 = iota((BLK, BLK), 1)
    eye = r0 == r1
    own = iota((BLK, ROWS), 1) == iota((BLK, ROWS), 0) + place * BLK

    def column(row):
        return jnp.sum(jnp.where(own, jnp.broadcast_to(row, (BLK, ROWS)), 0.0), axis=1, keepdims=True)

    def turned(col):
        return jnp.sum(jnp.where(eye, jnp.broadcast_to(col, (BLK, BLK)), 0.0), axis=0, keepdims=True)

    def before(row, col):
        hit = jnp.logical_and(row == col, r1 < r0)
        return jnp.sum(jnp.where(hit, 1.0, 0.0), axis=1, keepdims=True)

    group_col = column(group[...].astype(F32))
    group_row = turned(group_col)
    away = (group_col.astype(jnp.int32) - (z >> 1)) & 3
    near = jnp.where((z & 1) == 0, 3, 1)
    way = jnp.where(away == 0, 0, jnp.where(away == 2, 3, jnp.where(away == near, 1, 2)))
    where_to = way.astype(F32) * HALF_CAP + before(group_row, group_col)
    cols[...] = jnp.broadcast_to(where_to, (BLK, 128))
    rows[...] = jnp.broadcast_to(turned(where_to), (8, BLK))

    member_cols = [column(member[k : k + 1, :].astype(F32)) for k in range(2)]
    id_cols = [group_col * PER_GROUP + m for m in member_cols]
    id_rows = [turned(c) for c in id_cols]
    entries = []
    for k in range(2):
        rank = before(id_rows[0], id_cols[k]) + before(id_rows[1], id_cols[k])
        entries.append(member_cols[k] * PICK + rank + 1.0)
    for k in range(2):
        rest = column(weight[k : k + 1, :])
        for _ in range(3):
            part = rest.astype(BF16).astype(F32)
            entries.append(part)
            rest = rest - part
    lane = iota((BLK, 128), 1)
    table = jnp.zeros((BLK, 128), F32)
    for n, c in enumerate(entries):
        table = jnp.where(lane == n, c, table)
    table_out[...] = table.astype(BF16)
    own_copy.wait()


def project_kernel(att, weight, residual, gain, rows, table, normed_out, *refs):
    sent, matrix, sems = refs[:-2], refs[-2], refs[-1]
    copies = [
        pltpu.make_async_copy(weight.at[n * 256 : (n + 1) * 256, :], matrix.at[n], sems.at[n]) for n in range(4)
    ]
    for copy in copies:
        copy.start()
    summed = ALPHA * residual[...].astype(F32)
    for n, copy in enumerate(copies):
        copy.wait()
        summed += dot(jnp.concatenate([att[2 * n], att[2 * n + 1]], axis=1), matrix[n])
    mean_value = jnp.mean(summed, -1, keepdims=True)
    variance = jnp.mean(jnp.square(summed - mean_value), -1, keepdims=True)
    normed = ((summed - mean_value) * lax.rsqrt(variance + EPS) * gain[...]).astype(BF16)
    normed_out[...] = normed
    slot = iota((4 * HALF_CAP, BLK), 0).astype(F32)
    chosen = jnp.where(slot == rows[0:1, :], 1.0, 0.0).astype(BF16)
    picked = dot(chosen, normed).astype(BF16)
    tables = dot(chosen, table[...]).astype(BF16)
    for n, out in enumerate(sent):
        out[:, :D] = picked[n * HALF_CAP : (n + 1) * HALF_CAP]
        out[:, D:] = tables[n * HALF_CAP : (n + 1) * HALF_CAP]


def expand_kernel(first, second, out, table_out):
    eye = iota((HALF_CAP, HALF_CAP), 0) == iota((HALF_CAP, HALF_CAP), 1)
    slot = iota((CHUNK, HALF_CAP), 0).astype(F32)
    chosen = []
    for n, a in enumerate((first, second)):
        table = a[:, D:]
        table_out[n * HALF_CAP : (n + 1) * HALF_CAP, :] = table
        hit = None
        for k in range(2):
            col = table[:, k : k + 1].astype(F32)
            row = jnp.sum(jnp.where(eye, jnp.broadcast_to(col, eye.shape), 0.0), axis=0, keepdims=True)
            target = jnp.where(row > 0.5, row - 1.0 + n * CAP, -1.0)
            match = slot == target
            hit = match if hit is None else jnp.logical_or(hit, match)
        chosen.append(jnp.where(hit, 1.0, 0.0).astype(BF16))
    out[...] = (dot(chosen[0], first[:, :D]) + dot(chosen[1], second[:, :D])).astype(BF16)


def expert_kernel(order, x, *refs):
    weights, (out, gate, up, down, hidden, sems) = refs[: 2 * TP], refs[2 * TP :]
    moves = []
    for n in range(TP):
        head, tail = weights[2 * n], weights[2 * n + 1]
        moves.append((head.at[0:D, :], gate.at[n]))
        moves.append((head.at[D:, :], up.at[n, 0:FF]))
        moves.append((tail.at[0:FF, :], up.at[n, FF:D]))
    for n in range(TP):
        moves.append((weights[2 * n + 1].at[FF:, :], down.at[n]))
    copies = [pltpu.make_async_copy(a, b, sems.at[n]) for n, (a, b) in enumerate(moves)]
    for copy in copies:
        copy.start()
    for n in range(TP):
        for copy in copies[3 * n : 3 * n + 3]:
            copy.wait()
        both = dot(x[...], jnp.concatenate([gate[n], up[n]], axis=1))
        hidden[order[n]] = (jax.nn.silu(both[:, :128]) * both[:, 128:]).astype(BF16)
    units = jnp.concatenate([hidden[n] for n in range(TP)], axis=1)
    for n in range(TP):
        copies[3 * TP + n].wait()
        columns = jnp.concatenate([down[n, :FF, :], down[n, FF:, :]], axis=1)
        out[:, pl.ds(pl.multiple_of(order[n] * 256, 256), 256)] = dot(units, columns).astype(BF16)


def shrink_kernel(produced, table, first, second):
    count = 2 * HALF_CAP
    slot = iota((count, CHUNK), 1).astype(F32)
    origin = jnp.where(iota((count, 1), 0) >= HALF_CAP, float(CAP), 0.0)
    entries = table[...].astype(F32)
    total = jnp.zeros((count, D), F32)
    for k in range(2):
        col = entries[:, k : k + 1]
        target = jnp.where(col > 0.5, col - 1.0 + origin, -1.0)
        chosen = jnp.where(slot == target, 1.0, 0.0).astype(BF16)
        at = 2 + 3 * k
        weight = (entries[:, at : at + 1] + entries[:, at + 1 : at + 2]) + entries[:, at + 2 : at + 3]
        total += weight * dot(chosen, produced[...])
    first[...] = total[:HALF_CAP].astype(BF16)
    second[...] = total[HALF_CAP:].astype(BF16)


def combine_kernel(normed, cols, own, a, b, c, out):
    slot = iota((BLK, 4 * HALF_CAP), 1).astype(F32)
    chosen = jnp.where(slot == cols[:, 0:1], 1.0, 0.0).astype(BF16)
    stacked = jnp.concatenate([own[...], a[...], b[...], c[...]], axis=0)
    summed = ALPHA * normed[...].astype(F32) + dot(chosen, stacked)
    mean_value = jnp.mean(summed, -1, keepdims=True)
    variance = jnp.mean(jnp.square(summed - mean_value), -1, keepdims=True)
    scaled = (summed - mean_value) * lax.rsqrt(variance + EPS)
    width = out.shape[2]
    for n in range(out.shape[0]):
        out[n] = scaled[:, n * width : (n + 1) * width].astype(BF16)


def kernel(body, mib, outs, spaces, *operands, scratch=()):
    return pl.pallas_call(
        body,
        out_shape=outs,
        in_specs=spaces,
        out_specs=[VMEM] * len(outs),
        scratch_shapes=list(scratch),
        compiler_params=params(mib),
    )(*operands)


def layer(
    residual,
    queries,
    keys,
    values,
    segments,
    sink,
    out_weight,
    norm_gain_one,
    group,
    member,
    route_weight,
    gate_weight,
    up_weight,
    down_weight,
    norm_gain_two,
):
    place = lax.axis_index("tp")
    sp_place = lax.axis_index("sp")
    kt = keys.T
    vt = values.T
    seg = segments.reshape(BLOCKS, QB)
    halo = jax.ShapeDtypeStruct((144, HALF), BF16)
    packed_shape = pltpu.HBM((D + FF, 128), BF16)
    local = [jax.ShapeDtypeStruct(a.shape, a.dtype) for a in (queries, kt, vt, seg)]
    low, high, head, tail, queries, kt, vt, seg = pl.pallas_call(
        pack_kernel,
        out_shape=(halo, halo, packed_shape, packed_shape, *local),
        in_specs=[HBM] * 7,
        out_specs=(VMEM, VMEM, HBM, HBM) + (VMEM,) * 4,
        scratch_shapes=[pltpu.VMEM((2, D + FF, 128), BF16), pltpu.SemaphoreType.DMA((11,))],
        compiler_params=params(8),
        name="pack",
    )(*in_hbm(queries, kt, vt, seg, gate_weight, up_weight, down_weight))
    sp = SPX * SPZ
    forward = [(i, i + 1) for i in range(sp - 1)]
    before = lax.ppermute(high, "sp", forward)
    after = lax.ppermute(low, "sp", [(t, s) for s, t in forward])

    def along_y(array, shift):
        pairs = [(y * 2 + c, (y + shift) % 4 * 2 + c) for y in range(4) for c in range(2)]
        return lax.ppermute(array, "tp", pairs)

    def swapped(array):
        return lax.ppermute(array, "tp", [(n, n ^ 1) for n in range(TP)])

    from_low, from_high = along_y(head, 1), along_y(head, -1)
    tail_low, tail_high = along_y(tail, 1), along_y(tail, -1)
    head_far = along_y(from_low, 1)
    tail_far = along_y(tail_high, -1)
    other_heads = [swapped(a) for a in (head, from_low, from_high)]
    other_tails = [swapped(a) for a in (tail, tail_low, tail_high)]
    other_heads.append(swapped(head_far))
    other_tails.append(swapped(tail_far))
    heads_all = [head, from_low, from_high, head_far] + other_heads
    tails_all = [tail, tail_low, tail_high, tail_far] + other_tails
    weights = [a for pair in zip(heads_all, tails_all) for a in pair]

    rows_shape = jax.ShapeDtypeStruct((ROWS, 128), BF16)
    interior = pl.pallas_call(
        interior_kernel,
        out_shape=rows_shape,
        in_specs=[SMEM] + [VMEM] * 4,
        out_specs=VMEM,
        compiler_params=params(8),
        name="interior",
    )(sink, queries, kt, vt, seg)

    where = jnp.stack([place, sp_place >> 2]).astype(jnp.int32)
    rows, cols, table, own_residual = kernel(
        routing_kernel,
        12,
        (
            jax.ShapeDtypeStruct((8, BLK), F32),
            jax.ShapeDtypeStruct((BLK, 128), F32),
            jax.ShapeDtypeStruct((BLK, 128), BF16),
            jax.ShapeDtypeStruct((BLK, D), BF16),
        ),
        [SMEM] + [VMEM] * 3 + [HBM],
        where,
        group.reshape(1, ROWS),
        member.T,
        route_weight.T,
        *in_hbm(residual),
        scratch=[pltpu.SemaphoreType.DMA(())],
    )

    operands = (queries, kt, vt, seg, before, after, interior)
    attended = pl.pallas_call(
        edge_kernel,
        out_shape=rows_shape,
        in_specs=[SMEM] + [VMEM] * len(operands),
        out_specs=VMEM,
        compiler_params=params(8),
        name="edges",
    )(sink, *operands)

    heads = lax.all_to_all(attended.reshape(TP, BLK, 128), "tp", 0, 0, tiled=True)

    normed, *sent = kernel(
        project_kernel,
        24,
        [jax.ShapeDtypeStruct((BLK, D), BF16)] + [jax.ShapeDtypeStruct((HALF_CAP, WIDE), BF16)] * 4,
        [VMEM, HBM] + [VMEM] * 4,
        heads,
        *in_hbm(out_weight),
        own_residual,
        norm_gain_one.reshape(1, D),
        rows,
        table,
        scratch=[pltpu.VMEM((4, 256, D), BF16), pltpu.SemaphoreType.DMA((4,))],
    )

    def along_z(array, even, odd):
        step = (even, odd)
        pairs = [(z * SPX + x, (z + step[z % 2]) % SPZ * SPX + x) for z in range(SPZ) for x in range(SPX)]
        return lax.ppermute(array, "sp", pairs)

    def in_group(array):
        groups = [[g * GROUP + n for n in range(GROUP)] for g in range(sp // GROUP)]
        split = array.reshape(GROUP, PICK, D)
        moved = lax.all_to_all(split, "sp", 0, 0, axis_index_groups=groups, tiled=True)
        return moved.reshape(CHUNK, D)

    piece = jax.ShapeDtypeStruct((CHUNK, D), BF16)

    def spread(first, second):
        out = (piece, jax.ShapeDtypeStruct((2 * HALF_CAP, 128), BF16))
        rows, tables = kernel(expand_kernel, 12, out, [VMEM] * 2, first, second)
        return in_group(rows), tables

    def shrink(produced, tables):
        out = [jax.ShapeDtypeStruct((HALF_CAP, D), BF16)] * 2
        return kernel(shrink_kernel, 12, out, [VMEM] * 2, in_group(produced), tables)

    near = along_z(sent[1], -1, 1)
    other = along_z(sent[2], 2, -2)
    far = along_z(sent[3], -3, 3)
    rows_one, tables_one = spread(sent[0], near)
    rows_two, tables_two = spread(other, far)

    away = jnp.array([0, -2, 2, 4], jnp.int32)
    order = (jnp.concatenate([place + away, (place ^ 1) + away]) & 7).astype(jnp.int32)

    def apply(rows):
        return kernel(
            expert_kernel,
            24,
            (piece,),
            [SMEM, VMEM] + [HBM] * (2 * TP),
            order,
            rows,
            *in_hbm(*weights),
            scratch=[
                pltpu.VMEM((TP, D, 128), BF16),
                pltpu.VMEM((TP, D, 128), BF16),
                pltpu.VMEM((TP, D, 128), BF16),
                pltpu.VMEM((TP, CHUNK, 128), BF16),
                pltpu.SemaphoreType.DMA((4 * TP,)),
            ],
        )[0]

    made_one = apply(rows_one)
    made_two = apply(rows_two)
    back_two = shrink(made_two, tables_two)
    back_one = shrink(made_one, tables_one)
    back = [*back_one, *back_two]

    ret_near = along_z(back[1], -1, 1)
    ret_other = along_z(back[2], -2, 2)
    ret_far = along_z(back[3], -3, 3)

    (scaled,) = kernel(
        combine_kernel,
        16,
        (jax.ShapeDtypeStruct((TP, BLK, D // TP), BF16),),
        [VMEM] * 6,
        normed,
        cols,
        back[0],
        ret_near,
        ret_other,
        ret_far,
    )

    last = lax.all_to_all(scaled, "tp", 0, 0, tiled=True).reshape(ROWS, D // TP)
    return (last.astype(F32) * norm_gain_two).astype(BF16)


def solution(mesh):
    in_specs = (
        P("sp", None),
        P("sp", "tp"),
        P("sp", "tp"),
        P("sp", "tp"),
        P("sp"),
        P("tp"),
        P(),
        P(),
        P("sp"),
        P("sp", None),
        P("sp", None),
        P("sp", None, "tp"),
        P("sp", None, "tp"),
        P("sp", None, "tp"),
        P("tp"),
    )
    out_specs = P("sp", "tp")
    return jax.shard_map(layer, mesh=mesh, in_specs=in_specs, out_specs=out_specs, check_vma=False)
```
